32 devices in a mesh: sp: 16 (over z, y, x), tp: 2 (over core).
Axes of the slice: x: 2, y: 2, z: 4, core: 2. Of those that a mesh axis runs over, the one named last changes fastest.
Arguments:
- mixer_value_rows: bfloat16 [4096, 2048], P('sp', 'tp'), may hold values from -6 to 6
- input_map_rows: bfloat16 [4096, 256], P('sp', 'tp'), may hold values from -6 to 6
- output_map_rows: bfloat16 [4096, 256], P('sp', 'tp'), may hold values from -6 to 6
- gate_preactivation: bfloat16 [4096, 2048], P('sp', 'tp'), may hold values from -25 to 25
- step_preactivation: float32 [4096, 32], P('sp', 'tp'), may hold values from -4 to 4
- position_extra_decay: float32 [4096, 32], P('sp', 'tp'), may hold values from -0.69 to 0
- head_decay_rate: float32 [32], P('tp'), may hold values from 7.8125e-05 to 0.08
- head_direct_term: float32 [32], P('tp'), may hold values from -2.5 to 2.5
- value_taps: bfloat16 [4, 2048], P(None, 'tp'), may hold values from -3 to 3
- input_map_taps: bfloat16 [4, 256], P(None, 'tp'), may hold values from -3 to 3
- output_map_taps: bfloat16 [4, 256], P(None, 'tp'), may hold values from -3 to 3
- document_index: int32 [4096], P('sp'), may hold values from 0 to 3, never falling along the last dimension, each value on 1 to 1536 neighbouring positions
- gated_norm_gain: float32 [2048], replicated, may hold values from 0.1 to 1.9
- residual: bfloat16 [4096, 2048], P(('sp', 'tp')), may hold values from -6 to 6
- mixer_output_weight: bfloat16 [2048, 2048], replicated, may hold values from -0.125 to 0.125
- expert_norm_gain: float32 [2048], replicated, may hold values from 0.1 to 1.9
- expert_group_weight: float32 [4096, 4], P(('sp', 'tp')), may hold values from 0.5 to 2
- chosen_expert_weight: float32 [4096, 2], P(('sp', 'tp')), may hold values from 0.5 to 2
- chosen_expert_index: int32 [4096, 2], P(('sp', 'tp')), may hold values from 0 to 31, all different within a row; in each aligned block of 128 rows (0 to 127, 128 to 255, ...) at most 16 rows name the same one
- expert_gate_weight: bfloat16 [32, 2048, 512], P(('sp', 'tp')), may hold values from -0.125 to 0.125
- expert_up_weight: bfloat16 [32, 2048, 512], P(('sp', 'tp')), may hold values from -0.125 to 0.125
- expert_down_weight: bfloat16 [32, 512, 2048], P(('sp', 'tp')), may hold values from -0.25 to 0.25
Outputs:
- output: bfloat16 [4096, 2048], P(('sp', 'tp'))
The draws below stay inside these ranges and needn't reach their ends.
Inputs may be any that keep to these rules, and one draw needn't show every extreme that they name: `document_index`: document numbers never fall along the sequence; a document holds 1 to 1536 positions. `chosen_expert_index`: the 2 entries of a row differ. Among the rows of one device (aligned blocks of 128 rows) no expert is named by more than 16 rows, a bound that some expert reaches in some blocks.
All inputs are finite; a program needn't handle non-finite values.
Results may differ from the reference program's by a relative error of at most 0.019.
Values may be sent and summed in bfloat16 or wider, within the bound.
A program may use at most 128 MiB of HBM per device.

```python
import math
import jax
import jax.numpy as jnp
import numpy as np
from jax import lax

D = 2048
D_SSM = 2048
HEADS = 32
HEAD_DIM = 64
SSM_GROUPS = 2
D_STATE = 128
CONV_K = 4
BLOCK = 128
D_EXPERT = 512
EXPERT_GROUPS = 4
TOP = 2
TOK_DEV = 256
TOKENS = 4096
ROWS_DEV = 128
EXPERTS = 32
CAP = 16
N_SP = 16
N_TP = 2


def draw_gate_preactivation(key, part):
    position = jnp.arange(D_SSM, dtype=jnp.float32) / D_SSM
    scales = jnp.exp(1.6 * position)[None, :]
    values = jnp.clip(jax.random.normal(key, (TOKENS, D_SSM), jnp.float32), -4.9, 4.9)
    return (values * scales).astype(jnp.bfloat16)


def draw_step_preactivation(key, part):
    first, second = jax.random.split(key)
    blocks = TOKENS // TOK_DEV
    offsets = jax.random.uniform(second, (blocks, 1, 1), jnp.float32, -1.0, 1.0)
    noise = 0.7 * jnp.clip(jax.random.normal(first, (blocks, TOK_DEV, HEADS), jnp.float32), -4.0, 4.0)
    return (noise + offsets).reshape(TOKENS, HEADS)


def draw_head_decay_rate(key, part):
    first, second, third = jax.random.split(key, 3)
    share = 0.5
    slow_mask = jax.random.uniform(first, (HEADS,), jnp.float32) < share
    slow_rate = jnp.exp(jax.random.uniform(second, (HEADS,), jnp.float32, jnp.log(0.021 / TOK_DEV), jnp.log(0.2 / TOK_DEV)))
    fast_rate = jnp.exp(jax.random.uniform(third, (HEADS,), jnp.float32, jnp.log(0.021), jnp.log(0.079)))
    return jnp.where(slow_mask, slow_rate, fast_rate)


def draw_position_extra_decay(key, part):
    first, second = jax.random.split(key)
    hits = (jax.random.uniform(first, (TOKENS, 1), jnp.float32) < 24.0 / TOKENS).astype(jnp.float32)
    depth = jax.random.uniform(second, (TOKENS, HEADS), jnp.float32, 0.35, 0.69)
    return -depth * hits


def block_levels(own_key, extent, cuts, smallest, top_value):
    gain, own = 1.0, jax.random.fold_in(own_key, 6)
    for axis_at, blocks in cuts:
        heights = jnp.exp(jax.random.uniform(jax.random.fold_in(own, axis_at), (blocks,), jnp.float32, smallest / len(cuts), top_value / len(cuts)))
        gain = gain * jnp.repeat(heights, extent[axis_at] // blocks).reshape([-1 if axis == axis_at else 1 for axis in range(len(extent))])
    return gain


def split_up(number_of, total, reach, lean):
    loads = [(1 << 20) // math.isqrt(grade ** lean) + 1 for grade in range(2, number_of + 1)]
    rest, counts = total - reach - (number_of - 1), [1] * (number_of - 1)
    while rest > 0:
        movable = [i for i in range(number_of - 1) if counts[i] < reach]
        mass, left = sum([loads[i] for i in movable]), rest
        for i in movable:
            more = min(reach - counts[i], max(1, left * loads[i] // mass), rest)
            counts[i] = counts[i] + more
            rest = rest - more
    return np.array([reach] + counts)


def ragged(rng, amount, total, reach, lean):
    if amount == 2:
        one = jax.random.randint(rng, (), max(1, total - reach), min(reach, total - 1) + 1)
        return jnp.stack([one, total - one])
    tallies = jnp.asarray(split_up(amount, total, reach, lean), jnp.int32)
    couples = (amount - 1) // 2
    source_of, sink = tallies[1:1 + 2 * couples:2], tallies[2:2 + 2 * couples:2]
    margin = jnp.minimum(source_of - 1, reach - sink)
    moved = jax.random.randint(jax.random.fold_in(rng, 1), (couples,), 0, 1 << 20) % (margin + 1)
    tallies = tallies.at[1:1 + 2 * couples:2].set(source_of - moved).at[2:2 + 2 * couples:2].set(sink + moved)
    return tallies[jax.random.permutation(jax.random.fold_in(rng, 2), amount)]


def assign_block(key, own, number, rows, count, top, most, skew):
    sequence = jax.random.permutation(key, count)
    crowded, common = portions_of(count, rows * top, most, skew, True), portions_of(count, rows * top, most, skew, False)
    places = jnp.arange(count)

    def named(lengths, offset_by):
        used = int((lengths > 0).sum())
        fixed = max(1, used // 4)
        passed = fixed + (places - fixed + offset_by * (used - fixed)) % max(1, count - fixed)
        return jnp.zeros((count,), jnp.int32).at[sequence[jnp.where(places < fixed, places, passed)]].set(jnp.asarray(lengths, jnp.int32))

    lengths = jnp.where(number % 4 == 0, named(crowded, number // 4), named(common, number - number // 4 - 1))
    mixed = jax.random.permutation(jax.random.fold_in(own, 3), count)
    giver, receiver = mixed[0:count // 2 * 2:2], mixed[1:count // 2 * 2:2]
    slack = jnp.minimum(lengths[giver] - 1, most - lengths[receiver]) // 2
    slack = jnp.where((giver == sequence[0]) | (receiver == sequence[0]) | (lengths[receiver] == 0), 0, jnp.maximum(slack, 0))
    passed = jax.random.randint(jax.random.fold_in(own, 4), (count // 2,), 0, 1 << 20) % (slack + 1)
    lengths = lengths.at[giver].add(-passed).at[receiver].add(passed)
    members = jnp.searchsorted(jnp.cumsum(lengths), jnp.arange(rows * top), side="right").astype(jnp.int32)
    listing = members.reshape(top, rows).T
    listing = listing[jax.random.permutation(jax.random.fold_in(own, 1), rows)]
    offset_by = jax.random.randint(jax.random.fold_in(own, 2), (rows, 1), 0, top)
    return jnp.take_along_axis(listing, (jnp.arange(top)[None, :] + offset_by) % top, axis=1)


def portions_of(amount, total, limit, lean, full):
    portions = [(1 << 20) // math.isqrt(rank ** lean) + 1 for rank in range(1, amount + 1)]
    largest = limit if full else min(limit, max(-(-total // amount), total * portions[0] // sum(portions)))
    least = 1 if total - largest >= amount - 1 else 0
    holding, rest = [largest] + [least] * (amount - 1), total - largest - least * (amount - 1)
    while rest > 0:
        candidates = [i for i in range(1, amount) if holding[i] < largest] or [i for i in range(1, amount) if holding[i] < limit]
        pool, remaining = sum([portions[i] for i in candidates]), rest
        for i in candidates:
            more = min(limit - holding[i], max(1, remaining * portions[i] // pool), rest)
            holding[i] = holding[i] + more
            rest = rest - more
    return np.array(holding)


def centred(stream_key, dims, width, limit, cuts=(), kind=jnp.bfloat16):
    drawn = width * jax.random.normal(stream_key, dims, jnp.float32)
    if cuts:
        drawn = drawn * block_levels(stream_key, dims, cuts, -0.22, 0.18)
    return jnp.clip(drawn, -limit, limit).astype(kind)


def setup_inputs(seed: int = 0) -> dict:
    key_of = jax.random.split(jax.random.key(seed), 23)
    mixer_value_rows = centred(key_of[0], (TOKENS, D_SSM), 1.0, 6.0, ((0, 16), (1, 2)))
    input_map_rows = centred(key_of[1], (TOKENS, SSM_GROUPS * D_STATE), 1.0, 6.0, ((0, 16), (1, 2)))
    output_map_rows = centred(key_of[2], (TOKENS, SSM_GROUPS * D_STATE), 1.0, 6.0, ((0, 16), (1, 2)))
    gate_preactivation = draw_gate_preactivation(jax.random.fold_in(key_of[22], 71), 0)
    step_preactivation = draw_step_preactivation(jax.random.fold_in(key_of[22], 71), 0)
    position_extra_decay = draw_position_extra_decay(jax.random.fold_in(key_of[22], 71), 0)
    head_decay_rate = draw_head_decay_rate(jax.random.fold_in(key_of[22], 71), 0)
    head_direct_term = jnp.clip(jax.random.uniform(key_of[7], (HEADS,), jnp.float32, -2.5, 2.5) * block_levels(key_of[7], (HEADS,), ((0, 2),), -0.4, 0.0), -2.5, 2.5)
    value_taps = centred(key_of[8], (CONV_K, D_SSM), CONV_K ** -0.5, 3.0, ((1, 2),))
    input_map_taps = centred(key_of[9], (CONV_K, SSM_GROUPS * D_STATE), CONV_K ** -0.5, 3.0, ((1, 2),))
    output_map_taps = centred(key_of[10], (CONV_K, SSM_GROUPS * D_STATE), CONV_K ** -0.5, 3.0, ((1, 2),))
    document_index = jnp.searchsorted(jnp.cumsum(ragged(key_of[11], N_SP // 4, TOKENS, 6 * TOK_DEV, 1)), jnp.arange(TOKENS), side="right").astype(jnp.int32)
    gated_norm_gain = jnp.clip(1.0 + 0.18 * jax.random.normal(key_of[12], (D_SSM,), jnp.float32), 0.1, 1.9)
    residual = centred(key_of[13], (TOKENS, D), 1.0, 6.0, ((0, 32),))
    mixer_output_weight = centred(key_of[14], (D_SSM, D), D_SSM ** -0.5, 0.125)
    expert_norm_gain = jnp.clip(1.0 + 0.18 * jax.random.normal(key_of[15], (D,), jnp.float32), 0.1, 1.9)
    expert_group_weight = jnp.clip(0.5 + 1.5 * jax.random.uniform(key_of[16], (TOKENS, EXPERT_GROUPS), jnp.float32) ** block_levels(key_of[16], (TOKENS, EXPERT_GROUPS), ((0, 32),), -0.2, 0.2), 0.5, 2.0)
    chosen_expert_weight = jnp.clip(0.5 + 1.5 * jax.random.uniform(key_of[17], (TOKENS, TOP), jnp.float32) ** block_levels(key_of[17], (TOKENS, TOP), ((0, 32),), -0.2, 0.2), 0.5, 2.0)
    chosen_expert_index_keys = jax.random.split(jax.random.fold_in(key_of[18], 1), TOKENS // ROWS_DEV)
    chosen_expert_index_turns = jax.random.permutation(jax.random.fold_in(key_of[18], 3), TOKENS // ROWS_DEV)
    chosen_expert_index = jax.vmap(lambda own, number: assign_block(jax.random.fold_in(key_of[18], 2), own, number, ROWS_DEV, EXPERTS, TOP, CAP, 1))(chosen_expert_index_keys, chosen_expert_index_turns).reshape((TOKENS, TOP))
    expert_gate_weight = centred(key_of[19], (EXPERTS, D, D_EXPERT), D ** -0.5, 0.125, ((0, 32),))
    expert_up_weight = centred(key_of[20], (EXPERTS, D, D_EXPERT), D ** -0.5, 0.125, ((0, 32),))
    expert_down_weight = centred(key_of[21], (EXPERTS, D_EXPERT, D), D_EXPERT ** -0.5, 0.25, ((0, 32),))
    return dict(mixer_value_rows=mixer_value_rows, input_map_rows=input_map_rows, output_map_rows=output_map_rows, gate_preactivation=gate_preactivation, step_preactivation=step_preactivation, position_extra_decay=position_extra_decay, head_decay_rate=head_decay_rate, head_direct_term=head_direct_term, value_taps=value_taps, input_map_taps=input_map_taps, output_map_taps=output_map_taps, document_index=document_index, gated_norm_gain=gated_norm_gain, residual=residual, mixer_output_weight=mixer_output_weight, expert_norm_gain=expert_norm_gain, expert_group_weight=expert_group_weight, chosen_expert_weight=chosen_expert_weight, chosen_expert_index=chosen_expert_index, expert_gate_weight=expert_gate_weight, expert_up_weight=expert_up_weight, expert_down_weight=expert_down_weight)


EPSILON = 1e-06

def conv_silu(source_rows, weights, documents):
    kernel = weights.shape[0]
    length = source_rows.shape[0]
    padded = jnp.concatenate([jnp.zeros((kernel - 1, source_rows.shape[1]), jnp.float32), source_rows.astype(jnp.float32)], axis=0)
    pad_docs = jnp.concatenate([jnp.full((kernel - 1,), -1, jnp.int32), documents])
    summed = jnp.zeros((length, source_rows.shape[1]), jnp.float32)
    for offset in range(kernel):
        same_doc = (pad_docs[offset:offset + length] == documents).astype(jnp.float32)
        summed = summed + weights[offset].astype(jnp.float32)[None, :] * padded[offset:offset + length] * same_doc[:, None]
    return jax.nn.silu(summed).astype(jnp.bfloat16)

def scaled_norm(values, gain_vector):
    widened = values.astype(jnp.float32)
    factor = lax.rsqrt(lax.optimization_barrier(jnp.mean(widened * widened, axis=-1, keepdims=True)) + EPSILON)
    return (widened * factor * gain_vector.astype(jnp.float32)[None, :]).astype(jnp.bfloat16)

def block_step(carried_pair, pieces):
    carried, last_doc = carried_pair
    step_values, decay_block, b_block, c_block, doc_block = pieces
    length = step_values.shape[0]
    cumulative = jnp.cumsum(decay_block, axis=0)
    causal = jnp.arange(length)[:, None] >= jnp.arange(length)[None, :]
    allowed = causal & (doc_block[:, None] == doc_block[None, :])
    cum_heads = jnp.transpose(cumulative, (1, 2, 0))
    spread = cum_heads[:, :, :, None] - cum_heads[:, :, None, :]
    kernel_mat = jnp.exp(jnp.where(allowed[None, None], spread, -jnp.inf))
    scores = jnp.einsum('lgn,sgn->gls', c_block, b_block, preferred_element_type=jnp.float32)
    weighted = (scores[:, None] * kernel_mat).astype(jnp.bfloat16)
    inside = jnp.einsum('grls,sgrp->lgrp', weighted, step_values, preferred_element_type=jnp.float32)
    entering = (doc_block == last_doc).astype(jnp.float32)
    readout = jnp.einsum('lgn,grpn->lgrp', c_block, carried.astype(jnp.bfloat16), preferred_element_type=jnp.float32)
    inside = inside + readout * (jnp.exp(cumulative) * entering[:, None, None])[..., None]
    tail_mask = (doc_block == doc_block[-1]).astype(jnp.float32)
    end_decay = jnp.exp(cumulative[-1][None] - cumulative) * tail_mask[:, None, None]
    end_values = (end_decay[..., None] * step_values.astype(jnp.float32)).astype(jnp.bfloat16)
    fresh_state = jnp.einsum('lgn,lgrp->grpn', b_block, end_values, preferred_element_type=jnp.float32)
    keep_flag = (doc_block[-1] == last_doc).astype(jnp.float32)
    fresh_state = fresh_state + carried * (jnp.exp(cumulative[-1]) * keep_flag)[..., None, None]
    return ((fresh_state, doc_block[-1]), inside)

def state_mixer(value_conv, input_conv, output_conv, head_step_length, decay_logarithm, documents, head_direct_term):
    length = value_conv.shape[0]
    blocks = length // BLOCK
    per_group = HEADS // SSM_GROUPS
    value_heads = value_conv.astype(jnp.float32).reshape(length, SSM_GROUPS, per_group, HEAD_DIM)
    step_values = (value_heads * head_step_length.reshape(length, SSM_GROUPS, per_group)[..., None]).astype(jnp.bfloat16)
    decay_heads = decay_logarithm.reshape(blocks, BLOCK, SSM_GROUPS, per_group)
    input_groups = input_conv.reshape(blocks, BLOCK, SSM_GROUPS, D_STATE)
    output_groups = output_conv.reshape(blocks, BLOCK, SSM_GROUPS, D_STATE)
    doc_blocks = documents.reshape(blocks, BLOCK)
    initial = (jnp.zeros((SSM_GROUPS, per_group, HEAD_DIM, D_STATE), jnp.float32), jnp.array(-1, jnp.int32))
    ended, outputs = lax.scan(block_step, initial, (step_values.reshape(blocks, BLOCK, SSM_GROUPS, per_group, HEAD_DIM), decay_heads, input_groups, output_groups, doc_blocks))
    outputs = outputs.reshape(length, SSM_GROUPS, per_group, HEAD_DIM) + value_heads * head_direct_term.reshape(SSM_GROUPS, per_group)[None, :, :, None]
    return outputs.reshape(length, HEADS * HEAD_DIM)

def reference(mixer_value_rows, input_map_rows, output_map_rows, gate_preactivation, step_preactivation, position_extra_decay, head_decay_rate, head_direct_term, value_taps, input_map_taps, output_map_taps, document_index, gated_norm_gain, residual, mixer_output_weight, expert_norm_gain, expert_group_weight, chosen_expert_weight, chosen_expert_index, expert_gate_weight, expert_up_weight, expert_down_weight):
    documents = document_index.astype(jnp.int32)
    value_conv = conv_silu(mixer_value_rows, value_taps, documents)
    input_conv = conv_silu(input_map_rows, input_map_taps, documents)
    output_conv = conv_silu(output_map_rows, output_map_taps, documents)
    head_step_length = jax.nn.softplus(step_preactivation.astype(jnp.float32))
    decay_logarithm = position_extra_decay.astype(jnp.float32) - head_step_length * head_decay_rate.astype(jnp.float32)[None, :]
    mixer_out = state_mixer(value_conv, input_conv, output_conv, head_step_length, decay_logarithm, documents, head_direct_term.astype(jnp.float32))
    gated_rows = (mixer_out * jax.nn.silu(gate_preactivation.astype(jnp.float32))).astype(jnp.bfloat16)
    normed = scaled_norm(gated_rows, gated_norm_gain)
    mixed_rows = (residual.astype(jnp.float32) + jnp.dot(normed, mixer_output_weight, preferred_element_type=jnp.float32)).astype(jnp.bfloat16)
    ffn_in = scaled_norm(mixed_rows, expert_norm_gain)
    devices = N_SP * N_TP
    rows_dev = TOK_DEV // N_TP
    flat_ids = chosen_expert_index.astype(jnp.int32).reshape(devices, rows_dev * TOP)
    onehot = (flat_ids[:, :, None] == jnp.arange(EXPERTS, dtype=jnp.int32)[None, None, :]).astype(jnp.int32)
    ranking = lax.optimization_barrier(jnp.sum((jnp.cumsum(onehot, axis=1) - onehot) * onehot, axis=2))
    source = jnp.arange(devices, dtype=jnp.int32)[:, None]
    slot_index = (flat_ids * (devices * CAP) + source * CAP + ranking).reshape(-1)
    owners = jnp.arange(TOKENS * TOP, dtype=jnp.int32) // TOP
    slot_owner = jnp.zeros((EXPERTS * devices * CAP,), jnp.int32).at[slot_index].set(owners)
    slot_owner = slot_owner.reshape(EXPERTS, devices * CAP)

    def run_expert(pieces):
        indices, gate_matrix, up_matrix, down_matrix = pieces
        picked = ffn_in[indices]
        gate_part = jnp.dot(picked, gate_matrix, preferred_element_type=jnp.float32)
        upward = jnp.dot(picked, up_matrix, preferred_element_type=jnp.float32)
        hidden = (jax.nn.silu(gate_part) * upward).astype(jnp.bfloat16)
        return jnp.dot(hidden, down_matrix, preferred_element_type=jnp.float32).astype(jnp.bfloat16)
    results = lax.map(run_expert, (slot_owner, expert_gate_weight, expert_up_weight, expert_down_weight))
    gathered = results.reshape(-1, D)[slot_index].reshape(TOKENS, TOP, D)
    per_expert_group = EXPERTS // EXPERT_GROUPS
    owner_group = chosen_expert_index.astype(jnp.int32) // per_expert_group
    group_pick = (owner_group[:, :, None] == jnp.arange(EXPERT_GROUPS, dtype=jnp.int32)[None, None, :]).astype(jnp.float32)
    route_weight = lax.optimization_barrier(jnp.sum(group_pick * expert_group_weight[:, None, :], axis=2)) * chosen_expert_weight
    summed = mixed_rows.astype(jnp.float32) + lax.optimization_barrier(jnp.sum(route_weight[:, :, None] * gathered.astype(jnp.float32), axis=1))
    return summed.astype(jnp.bfloat16)
```

```python
import functools

import jax
import jax.numpy as jnp
import numpy as np
from jax import lax
from jax.experimental import pallas as pl
from jax.experimental.pallas import tpu as pltpu
from jax.sharding import PartitionSpec as P

D_STATE = 128
EXPERT_GROUPS = 4
LONGEST = 1536
EPSILON = 1e-06

NEG = -1e30
MESH_ID = pl.DeviceIdType.MESH
OFFSETS = (1, 2, 5)


def softplus(v):
    return jnp.maximum(v, 0.0) + jnp.log1p(jnp.exp(-jnp.abs(v)))


def silu(v):
    return v / (1.0 + jnp.exp(-v))


def exact_dot(a, b):
    return jnp.dot(a, b, preferred_element_type=jnp.float32, precision=lax.Precision.HIGHEST)


def mixer_kernel(
    n, x_hbm, b_hbm, c_hbm, gate_hbm, step_hbm, extra_hbm, docs_hbm, resid_hbm, w_hbm,
    rate_ref, direct_ref, spread_ref, taps_ref, btaps_ref, ctaps_ref, docrow_ref, gain_ref,
    gain2_ref,
    mixed_ref, ffn_ref,
    x_ref, b_ref, c_ref, gate_ref, step_ref, extra_ref, docs_ref, resid_ref, w_ref, pad, pad_docs, edge_x, edge_b, edge_c, edge_d,
    vconv, bconv, cconv, ylocal, cumx, s32, t0, t1, t2, g0, g1, g2,
    r0, r1, r1far, r2, rg0, rg1, rg2, gated, regrouped,
    wsem, send, recv,
):
    sp = lax.axis_index("sp")
    tp = lax.axis_index("tp")
    length, channels = x_ref.shape
    state = b_ref.shape[1]
    lanes = 128
    chunks = channels // lanes
    heads = step_ref.shape[1]
    half = length // 2
    edge = edge_x.shape[0]

    loads = [
        pltpu.make_async_copy(source, target, wsem.at[i])
        for i, (source, target) in enumerate((
            (x_hbm, x_ref), (b_hbm, b_ref), (c_hbm, c_ref), (docs_hbm, docs_ref),
            (step_hbm, step_ref), (extra_hbm, extra_ref), (gate_hbm, gate_ref),
            (resid_hbm, resid_ref), (w_hbm, w_ref),
        ))
    ]
    for load in loads:
        load.start()

    barrier = pltpu.get_barrier_semaphore()
    count = jnp.int32(1)
    pl.semaphore_signal(barrier, inc=1, device_id=(sp, 1 - tp), device_id_type=MESH_ID)
    for off in OFFSETS:
        @pl.when(sp + off < n)
        def _():
            pl.semaphore_signal(barrier, inc=1, device_id=(sp + off, tp), device_id_type=MESH_ID)

        @pl.when(sp >= off)
        def _():
            pl.semaphore_signal(barrier, inc=1, device_id=(sp - off, tp), device_id_type=MESH_ID)

        count = count + (sp + off < n).astype(jnp.int32) + (sp >= off).astype(jnp.int32)
    pl.semaphore_wait(barrier, count)

    def copy(slot, src, dst, off):
        return pltpu.make_async_remote_copy(
            src_ref=src, dst_ref=dst, send_sem=send.at[slot], recv_sem=recv.at[slot],
            device_id=(sp + off, tp), device_id_type=MESH_ID,
        )

    last = pl.ds(length - edge, edge)
    edges = [
        copy(0, x_ref.at[last, :], edge_x, 1),
        copy(1, b_ref.at[last, :], edge_b, 1),
        copy(2, c_ref.at[last, :], edge_c, 1),
        copy(3, docs_ref.at[last, :], edge_d, 1),
    ]

    def start(copies, off):
        @pl.when(sp + off < n)
        def _():
            for one in copies:
                one.start()

    def wait_recv(copies, off):
        @pl.when(sp >= off)
        def _():
            for one in copies:
                one.wait_recv()

    def wait_send(copies, off):
        @pl.when(sp + off < n)
        def _():
            for one in copies:
                one.wait_send()

    for load in loads[:4]:
        load.wait()
    start(edges, 1)
    for load in loads[4:6]:
        load.wait()

    step = softplus(step_ref[...])
    logs = extra_ref[...] - step * rate_ref[...]
    rows = lax.broadcasted_iota(jnp.int32, (length, length), 0)
    cols = lax.broadcasted_iota(jnp.int32, (length, length), 1)
    causal = rows >= cols
    cum = exact_dot(causal.astype(jnp.float32), logs)
    cum_t = lax.dot_general(
        logs, (rows <= cols).astype(jnp.float32), (((0,), (0,)), ((), ())),
        preferred_element_type=jnp.float32, precision=lax.Precision.HIGHEST,
    )
    same = docs_ref[:, 0:1] == docrow_ref[0:1, :]
    blocked = jnp.where(causal & same, 0.0, NEG)
    tail = (docs_ref[...] == docs_ref[length - 1 : length, :]).astype(jnp.float32)

    pad[edge:, :channels] = x_ref[...].astype(jnp.float32)
    pad[edge:, channels : channels + state] = b_ref[...].astype(jnp.float32)
    pad[edge:, channels + state :] = c_ref[...].astype(jnp.float32)
    pad_docs[edge:, :] = docs_ref[...]

    wait_recv(edges, 1)
    has = sp >= 1
    pad[:edge, :channels] = jnp.where(has, edge_x[...].astype(jnp.float32), 0.0)
    pad[:edge, channels : channels + state] = jnp.where(has, edge_b[...].astype(jnp.float32), 0.0)
    pad[:edge, channels + state :] = jnp.where(has, edge_c[...].astype(jnp.float32), 0.0)
    pad_docs[:edge, :] = jnp.where(has, edge_d[...], 0.0)

    taps_count = taps_ref.shape[0]
    base = edge - taps_count + 1
    masks = [
        (pad_docs[base + k : base + k + length, :] == docs_ref[...]).astype(jnp.float32)
        for k in range(taps_count - 1)
    ]

    def conv(at, taps, start_lane):
        total = taps[taps_count - 1 :, start_lane : start_lane + lanes].astype(
            jnp.float32
        ) * pad[edge : edge + length, at : at + lanes]
        for k in range(taps_count - 1):
            total = total + (
                taps[k : k + 1, start_lane : start_lane + lanes].astype(jnp.float32)
                * pad[base + k : base + k + length, at : at + lanes]
                * masks[k]
            )
        return silu(total).astype(jnp.bfloat16)

    bconv[...] = conv(channels, btaps_ref, 0)
    cconv[...] = conv(channels + state, ctaps_ref, 0)

    keep = (docs_ref[length - 1 : length, :] == pad_docs[edge - 1 : edge, :]).astype(jnp.float32)
    keep = keep * has.astype(jnp.float32)
    b_t = jnp.transpose(bconv[...].astype(jnp.float32)).astype(jnp.bfloat16)
    for j in range(chunks):
        at = slice(j * lanes, (j + 1) * lanes)
        value = conv(j * lanes, taps_ref, j * lanes)
        vconv[:, at] = value
        widen = spread_ref[:, at]
        cum_wide = exact_dot(cum, widen)
        cumx[:, at] = cum_wide
        stepped = (exact_dot(step, widen) * value.astype(jnp.float32)).astype(jnp.bfloat16)
        ylocal[:, at] = stepped.astype(jnp.float32)
        ending = cum_wide[length - 1 : length, :]
        ended = (jnp.exp(ending - cum_wide) * tail * stepped.astype(jnp.float32)).astype(
            jnp.bfloat16
        )
        fresh = jnp.dot(b_t, ended, preferred_element_type=jnp.float32)
        s32[:, at] = fresh
        t0[:, at] = fresh.astype(jnp.bfloat16)
        g0[:, at] = jnp.broadcast_to(jnp.exp(ending) * keep, (8, lanes))
    first = [copy(4, t0, r0, 1), copy(5, g0, rg0, 1)]
    start(first, 1)

    scores = lax.dot_general(
        cconv[...], bconv[...], (((1,), (1,)), ((), ())), preferred_element_type=jnp.float32
    )
    per_chunk = heads // chunks
    width = lanes // per_chunk
    lane = lax.broadcasted_iota(jnp.int32, (length, lanes), 1)

    def inside(j):
        at = slice(j * lanes, (j + 1) * lanes)
        stepped = ylocal[:, at].astype(jnp.bfloat16)
        result = None
        for k in range(per_chunk):
            h = j * per_chunk + k
            decay = jnp.exp(cum[:, h : h + 1] - cum_t[h : h + 1, :] + blocked)
            part = jnp.dot(
                (scores * decay).astype(jnp.bfloat16), stepped, preferred_element_type=jnp.float32
            )
            result = part if result is None else jnp.where(lane < k * width, result, part)
        direct = direct_ref[:, at]
        ylocal[:, at] = result + direct * vconv[:, at].astype(jnp.float32)

    third = chunks // 3
    for j in range(third):
        inside(j)

    wait_recv(first, 1)
    grow0 = g0[0:1, :]
    before = jnp.where(has, r0[...].astype(jnp.float32), 0.0)
    s32[...] = s32[...] + grow0 * before
    t1[...] = s32[...].astype(jnp.bfloat16)
    g1[...] = g0[...] * jnp.where(has, rg0[...], 0.0)
    second = [copy(6, t1, r1, 2), copy(7, g1, rg1, 2)]
    far = [copy(8, t1, r1far, 5)]
    start(second, 2)
    start(far, 5)
    for j in range(third, 2 * third):
        inside(j)

    wait_recv(second, 2)
    has2 = sp >= 2
    before = jnp.where(has2, r1[...].astype(jnp.float32), 0.0)
    t2[...] = (s32[...] + g1[0:1, :] * before).astype(jnp.bfloat16)
    g2[...] = g1[...] * jnp.where(has2, rg1[...], 0.0)
    final = [copy(9, t2, r2, 1), copy(10, g2, rg2, 1)]
    start(final, 1)
    for j in range(2 * third, chunks):
        inside(j)

    wait_recv(final, 1)
    wait_recv(far, 5)
    has5 = sp >= 5
    incoming = (
        jnp.where(has, r2[...].astype(jnp.float32), 0.0)
        + jnp.where(has, rg2[0:1, :], 0.0) * jnp.where(has5, r1far[...].astype(jnp.float32), 0.0)
    ).astype(jnp.bfloat16)
    loads[6].wait()
    entering = (docs_ref[...] == pad_docs[edge - 1 : edge, :]).astype(jnp.float32)
    for j in range(chunks):
        at = slice(j * lanes, (j + 1) * lanes)
        readout = jnp.dot(cconv[...], incoming[:, at], preferred_element_type=jnp.float32)
        whole = ylocal[:, at] + readout * jnp.exp(cumx[:, at]) * entering
        gated[:, at] = (whole * silu(gate_ref[:, at].astype(jnp.float32))).astype(jnp.bfloat16)

    swap = pltpu.make_async_remote_copy(
        src_ref=gated.at[pl.ds(pl.multiple_of((1 - tp) * half, half), half), :],
        dst_ref=regrouped,
        send_sem=send.at[11], recv_sem=recv.at[11],
        device_id=(sp, 1 - tp), device_id_type=MESH_ID,
    )
    swap.start()
    wait_send(edges, 1)
    wait_send(first, 1)
    wait_send(second, 2)
    wait_send(far, 5)
    wait_send(final, 1)
    loads[7].wait()
    loads[8].wait()
    swap.wait()
    own = gated[pl.ds(pl.multiple_of(tp * half, half), half), :].astype(jnp.float32)
    other = regrouped[...].astype(jnp.float32)
    total = jnp.sum(own * own, axis=-1, keepdims=True) + jnp.sum(other * other, axis=-1, keepdims=True)
    features = 2 * channels
    factor = lax.rsqrt(total / features + EPSILON)
    low = jnp.where(tp == 0, own, other)
    high = jnp.where(tp == 0, other, own)
    low = (low * factor * gain_ref[:, :channels]).astype(jnp.bfloat16)
    high = (high * factor * gain_ref[:, channels:]).astype(jnp.bfloat16)
    square = jnp.zeros((half, 1), jnp.float32)
    piece = 512
    model = resid_ref.shape[1]
    for j in range(model // piece):
        at = slice(j * piece, (j + 1) * piece)
        projected = jnp.dot(low, w_ref[:channels, at], preferred_element_type=jnp.float32)
        projected += jnp.dot(high, w_ref[channels:, at], preferred_element_type=jnp.float32)
        mixed = (resid_ref[:, at].astype(jnp.float32) + projected).astype(jnp.bfloat16)
        mixed_ref[:, at] = mixed
        wide = mixed.astype(jnp.float32)
        square += jnp.sum(wide * wide, axis=-1, keepdims=True)
    factor = lax.rsqrt(square / model + EPSILON)
    ffn_ref[...] = (mixed_ref[...].astype(jnp.float32) * factor * gain2_ref[...]).astype(jnp.bfloat16)


def mixer(n, x, b, c, gate, step, extra, rate, direct, taps, btaps, ctaps, docs, gain, resid,
          weight, gain2):
    length, channels = x.shape
    state = b.shape[1]
    heads = step.shape[1]
    width = channels // heads
    model = resid.shape[1]
    half = resid.shape[0]
    assert state == D_STATE and (LONGEST - 2) // length + 1 <= 6
    marks = (docs + 1).astype(jnp.float32)
    docs_wide = jnp.broadcast_to(marks[:, None], (length, 128))
    docs_row = jnp.broadcast_to(marks[None, :], (8, length))
    spread = jnp.asarray(np.repeat(np.eye(heads, dtype=np.float32), width, axis=1))
    direct_wide = jnp.repeat(direct, width)[None, :]
    bf, f32 = jnp.bfloat16, jnp.float32
    edge = 16
    vm = pltpu.VMEM
    return pl.pallas_call(
        functools.partial(mixer_kernel, n),
        out_shape=[jax.ShapeDtypeStruct((half, model), bf)] * 2,
        in_specs=[pl.BlockSpec(memory_space=pl.ANY)] * 9
        + [pl.BlockSpec(memory_space=pltpu.VMEM)] * 9,
        out_specs=[pl.BlockSpec(memory_space=pltpu.VMEM)] * 2,
        scratch_shapes=[
            vm(x.shape, bf), vm(b.shape, bf), vm(c.shape, bf), vm(gate.shape, bf),
            vm(step.shape, f32), vm(extra.shape, f32), vm(docs_wide.shape, f32),
            vm(resid.shape, bf), vm(weight.shape, bf),
            vm((edge + length, channels + 2 * state), f32), vm((edge + length, 128), f32),
            vm((edge, channels), bf), vm((edge, state), bf), vm((edge, state), bf),
            vm((edge, 128), f32),
            vm((length, channels), bf), vm((length, state), bf), vm((length, state), bf),
            vm((length, channels), f32), vm((length, channels), f32),
            vm((state, channels), f32),
            vm((state, channels), bf), vm((state, channels), bf), vm((state, channels), bf),
            vm((8, channels), f32), vm((8, channels), f32), vm((8, channels), f32),
            vm((state, channels), bf), vm((state, channels), bf), vm((state, channels), bf),
            vm((state, channels), bf),
            vm((8, channels), f32), vm((8, channels), f32), vm((8, channels), f32),
            vm((length, channels), bf), vm((half, channels), bf),
            pltpu.SemaphoreType.DMA((9,)), pltpu.SemaphoreType.DMA((12,)), pltpu.SemaphoreType.DMA((12,)),
        ],
        compiler_params=pltpu.CompilerParams(
            collective_id=0, has_side_effects=True, vmem_limit_bytes=58 * 1024 * 1024
        ),
    )(x, b, c, gate, step, extra, docs_wide, resid, weight, rate[None, :], direct_wide, spread,
      taps, btaps, ctaps, docs_row, gain[None, :], gain2[None, :])


def plane_kernel(
    planes, tps, ffn_ref, ids_ref, group_ref, weight_ref, mixed_ref, wg_hbm, wu_hbm, wd_hbm,
    out_ref,
    wg, wu, wd, meta, picks, routes, line, slots, arrived, done, back, part, mine, parts,
    wsem, msend, mrecv, lsend, lrecv, fsend, frecv, bsend, brecv, psend, precv,
):
    sp = lax.axis_index("sp")
    tp = lax.axis_index("tp")
    rows, model = ffn_ref.shape
    per = lax.axis_size("sp") * tps // planes
    hosts = per // tps
    cap = rows // per
    experts = planes * per
    chunks = lrecv.shape[1]
    width = model // chunks
    z = sp // hosts
    q = (sp % hosts) * tps + tp

    loads = [
        pltpu.make_async_copy(wg_hbm.at[0], wg, wsem.at[0]),
        pltpu.make_async_copy(wu_hbm.at[0], wu, wsem.at[1]),
        pltpu.make_async_copy(wd_hbm.at[0], wd, wsem.at[2]),
    ]
    for load in loads:
        load.start()

    def place(plane, member):
        return (plane * hosts + member // tps, member % tps)

    def loop(low, high, act):
        def body(k, carry):
            act(k)
            return carry

        lax.fori_loop(low, high, body, 0)

    barrier = pltpu.get_barrier_semaphore()

    def greet(device):
        pl.semaphore_signal(barrier, inc=1, device_id=device, device_id_type=MESH_ID)

    loop(1, per, lambda d: greet(place(z, (q + d) % per)))
    loop(1, planes, lambda d: greet(place((z + d) % planes, q)))

    def columns(c):
        return pl.ds(pl.multiple_of(c * width, width), width)

    def member_rows(member):
        return pl.ds(pl.multiple_of(member * cap, cap), cap)

    def tell(plane, target):
        return pltpu.make_async_remote_copy(
            src_ref=meta.at[plane], dst_ref=meta.at[plane],
            send_sem=msend.at[target], recv_sem=mrecv.at[plane],
            device_id=place(target, q), device_id_type=MESH_ID,
        )

    def hop(plane, c, up):
        return pltpu.make_async_remote_copy(
            src_ref=line.at[plane, :, columns(c)], dst_ref=line.at[plane, :, columns(c)],
            send_sem=lsend.at[up, plane, c], recv_sem=lrecv.at[plane, c],
            device_id=place(z + 2 * up - 1, q), device_id_type=MESH_ID,
        )

    def forward(plane, c, member):
        return pltpu.make_async_remote_copy(
            src_ref=slots.at[plane, member_rows(member), columns(c)],
            dst_ref=arrived.at[plane, member_rows(q), columns(c)],
            send_sem=fsend.at[plane], recv_sem=frecv.at[plane],
            device_id=place(z, member), device_id_type=MESH_ID,
        )

    def backward(plane, c, member):
        return pltpu.make_async_remote_copy(
            src_ref=done.at[plane, member_rows(member), columns(c)],
            dst_ref=back.at[plane, member_rows(q), columns(c)],
            send_sem=bsend.at[plane], recv_sem=brecv.at[plane, c],
            device_id=place(z, member), device_id_type=MESH_ID,
        )

    def home(plane, c):
        return pltpu.make_async_remote_copy(
            src_ref=part.at[plane, :, columns(c)], dst_ref=parts.at[z, :, columns(c)],
            send_sem=psend.at[plane, c], recv_sem=precv.at[z, c],
            device_id=place(plane, q), device_id_type=MESH_ID,
        )

    def homed(plane, c):
        return pltpu.make_async_copy(
            parts.at[plane, :, columns(c)], parts.at[plane, :, columns(c)], precv.at[plane, c]
        )

    others = pl.ds(0, (per - 1) * cap)

    def whole(ref, plane, sem):
        view = ref.at[plane, others, :]
        return pltpu.make_async_copy(view, view, sem.at[plane])

    def slab(plane, c):
        view = back.at[plane, others, columns(c)]
        return pltpu.make_async_copy(view, view, brecv.at[plane, c])

    line[z] = ffn_ref[...]
    ids = ids_ref[...]
    group_size = experts // EXPERT_GROUPS
    weight = jnp.zeros(ids.shape, jnp.float32)
    for g in range(EXPERT_GROUPS):
        inside = (ids >= g * group_size) & (ids < (g + 1) * group_size)
        weight = weight + jnp.where(inside, group_ref[g : g + 1, :], 0.0)
    choose = ids.shape[0]
    info = jnp.concatenate(
        [
            ids.astype(jnp.float32), weight * weight_ref[...],
            jnp.zeros((meta.shape[1] - 2 * choose, rows), jnp.float32),
        ],
        axis=0,
    )
    meta[z] = info
    pl.semaphore_wait(barrier, per + planes - 2)
    loop(1, planes, lambda d: tell(z, (z + d) % planes).start())
    for c in range(chunks):
        @pl.when(z < planes - 1)
        def _():
            hop(z, c, 1).start()

        @pl.when(z > 0)
        def _():
            hop(z, c, 0).start()

    slot_member = lax.broadcasted_iota(jnp.int32, (per, cap, rows), 0).reshape(rows, rows)
    slot_place = lax.broadcasted_iota(jnp.int32, (per, cap, rows), 1).reshape(rows, rows)
    slot_expert = (slot_member + z * per).astype(jnp.float32)
    slot_place = slot_place.astype(jnp.float32)
    earlier = (
        lax.broadcasted_iota(jnp.int32, (rows, rows), 0)
        < lax.broadcasted_iota(jnp.int32, (rows, rows), 1)
    ).astype(jnp.bfloat16)

    def sort_out(plane):
        known = meta[plane]
        named = jnp.zeros((rows, rows), jnp.float32)
        value = jnp.zeros((rows, rows), jnp.float32)
        for k in range(choose):
            chosen = (known[k : k + 1, :] == slot_expert).astype(jnp.float32)
            named = named + chosen
            value = value + chosen * known[choose + k : choose + k + 1, :]
        rank = jnp.dot(named.astype(jnp.bfloat16), earlier, preferred_element_type=jnp.float32)
        hot = jnp.where(rank == slot_place, named, 0.0)
        picks[plane] = hot.astype(jnp.bfloat16)
        routes[plane] = jnp.transpose(hot * value).astype(jnp.bfloat16)

    lag = chunks + 2

    def stage_rows(k, c, up, plane):
        @pl.when(k > 0)
        def _():
            hop(plane, c, up).wait_recv()

            @pl.when((up == 0) & (z < planes - 1))
            def _():
                hop(plane, c, 1).start()

            @pl.when((up == 1) & (z > 0))
            def _():
                hop(plane, c, 0).start()

        @pl.when(c == 0)
        def _():
            @pl.when(k > 0)
            def _():
                tell(plane, plane).wait_recv()

            sort_out(plane)

        at = columns(c)
        slots[plane, :, at] = jnp.dot(
            picks[plane], line[plane, :, at], preferred_element_type=jnp.float32
        ).astype(jnp.bfloat16)
        arrived[plane, member_rows(q), at] = slots[plane, member_rows(q), at]
        loop(1, per, lambda d: forward(plane, c, (q + d) % per).start())

    def stage_experts(k, plane):
        @pl.when(k == 0)
        def _():
            for load in loads:
                load.wait()

        whole(arrived, plane, frecv).wait()
        tokens = arrived[plane]
        gate = jnp.dot(tokens, wg[...], preferred_element_type=jnp.float32)
        up = jnp.dot(tokens, wu[...], preferred_element_type=jnp.float32)
        hidden = (silu(gate) * up).astype(jnp.bfloat16)
        for c in range(chunks):
            at = slice(c * width, (c + 1) * width)
            done[plane, :, at] = jnp.dot(
                hidden, wd[:, at], preferred_element_type=jnp.float32
            ).astype(jnp.bfloat16)
            back[plane, member_rows(q), at] = done[plane, member_rows(q), at]
            loop(1, per, lambda d: backward(plane, c, (q + d) % per).start())

    def stage_home(k, c, plane):
        slab(plane, c).wait()
        at = columns(c)
        total = jnp.dot(
            routes[plane], back[plane, :, at], preferred_element_type=jnp.float32
        )

        @pl.when(k == 0)
        def _():
            mine[:, at] = total

        @pl.when(k > 0)
        def _():
            part[plane, :, at] = total.astype(jnp.bfloat16)
            home(plane, c).start()

    def tick(v):
        def both(k, act):
            def side(up):
                plane = z + k * (2 * up - 1)

                @pl.when((plane >= 0) & (plane < planes) & ((k > 0) | (up == 0)))
                def _():
                    act(up, plane)

            loop(0, 2, side)

        @pl.when(v < planes * chunks)
        def _():
            k = v // chunks
            c = v % chunks
            both(k, lambda up, plane: stage_rows(k, c, up, plane))

        @pl.when((v % chunks == 0) & (v >= chunks) & (v <= planes * chunks))
        def _():
            k = v // chunks - 1
            both(k, lambda up, plane: stage_experts(k, plane))

        @pl.when(v >= lag)
        def _():
            k = (v - lag) // chunks
            c = (v - lag) % chunks
            both(k, lambda up, plane: stage_home(k, c, plane))

    loop(0, planes * chunks + lag, tick)

    for c in range(chunks):
        at = slice(c * width, (c + 1) * width)
        loop(1, planes, lambda d: homed((z + d) % planes, c).wait())
        mine[:, at] = mine[:, at] + mixed_ref[:, at].astype(jnp.float32)

        def add(d):
            mine[:, at] = mine[:, at] + parts[(z + d) % planes, :, at].astype(jnp.float32)

        loop(1, planes, add)
        out_ref[:, at] = mine[:, at].astype(jnp.bfloat16)

    loop(1, planes, lambda d: tell(z, (z + d) % planes).wait_send())

    def finish(plane):
        whole(slots, plane, fsend).wait()
        whole(done, plane, bsend).wait()

        def each(c):
            @pl.when((plane <= z) & (z < planes - 1))
            def _():
                hop(plane, c, 1).wait_send()

            @pl.when((plane >= z) & (z > 0))
            def _():
                hop(plane, c, 0).wait_send()

            @pl.when(plane != z)
            def _():
                home(plane, c).wait_send()

        loop(0, chunks, each)

    loop(0, planes, finish)


def exchange(ffn, ids, group_weight, chosen_weight, mixed, gate_weight, up_weight, down_weight,
             planes):
    rows, model = ffn.shape
    chunks = 4
    bf, f32 = jnp.bfloat16, jnp.float32
    vm = pltpu.VMEM
    dma = pltpu.SemaphoreType.DMA
    return pl.pallas_call(
        functools.partial(plane_kernel, planes, lax.axis_size("tp")),
        out_shape=jax.ShapeDtypeStruct(mixed.shape, bf),
        in_specs=[pl.BlockSpec(memory_space=pltpu.VMEM)] * 5
        + [pl.BlockSpec(memory_space=pl.ANY)] * 3,
        out_specs=pl.BlockSpec(memory_space=pltpu.VMEM),
        scratch_shapes=[
            vm(gate_weight.shape[1:], bf), vm(up_weight.shape[1:], bf),
            vm(down_weight.shape[1:], bf),
            vm((planes, 8, rows), f32),
            vm((planes, rows, rows), bf), vm((planes, rows, rows), bf),
            vm((planes, rows, model), bf), vm((planes, rows, model), bf),
            vm((planes, rows, model), bf), vm((planes, rows, model), bf),
            vm((planes, rows, model), bf), vm((planes, rows, model), bf),
            vm((rows, model), f32), vm((planes, rows, model), bf),
            dma((3,)), dma((planes,)), dma((planes,)),
            dma((2, planes, chunks)), dma((planes, chunks)),
            dma((planes,)), dma((planes,)), dma((planes,)), dma((planes, chunks)),
            dma((planes, chunks)), dma((planes, chunks)),
        ],
        compiler_params=pltpu.CompilerParams(
            collective_id=1, has_side_effects=True, vmem_limit_bytes=56 * 1024 * 1024
        ),
    )(ffn, ids, group_weight, chosen_weight, mixed, gate_weight, up_weight, down_weight)


def local(
    mixer_value_rows,
    input_map_rows,
    output_map_rows,
    gate_preactivation,
    step_preactivation,
    position_extra_decay,
    head_decay_rate,
    head_direct_term,
    value_taps,
    input_map_taps,
    output_map_taps,
    document_index,
    gated_norm_gain,
    residual,
    mixer_output_weight,
    expert_norm_gain,
    expert_group_weight,
    chosen_expert_weight,
    chosen_expert_index,
    expert_gate_weight,
    expert_up_weight,
    expert_down_weight,
):
    mixed_rows, ffn_in = mixer(
        lax.axis_size("sp"), mixer_value_rows, input_map_rows, output_map_rows,
        gate_preactivation, step_preactivation, position_extra_decay, head_decay_rate,
        head_direct_term, value_taps, input_map_taps, output_map_taps, document_index,
        gated_norm_gain, residual, mixer_output_weight, expert_norm_gain,
    )
    experts = lax.axis_size("sp") * lax.axis_size("tp")
    row_count, width = ffn_in.shape
    choose = chosen_expert_index.shape[1]
    capacity = 2 * mixer_value_rows.shape[0] // experts
    per = row_count // capacity
    if (
        capacity % 16 == 0 and row_count % capacity == 0 and experts % per == 0
        and per % lax.axis_size("tp") == 0 and experts % EXPERT_GROUPS == 0 and choose <= 4
    ):
        return exchange(
            ffn_in, chosen_expert_index.T, expert_group_weight.T, chosen_expert_weight.T,
            mixed_rows, expert_gate_weight, expert_up_weight, expert_down_weight, experts // per,
        )
    ids = jnp.arange(experts, dtype=jnp.int32)
    chosen = (chosen_expert_index[:, :, None] == ids).astype(jnp.bfloat16)
    named = jnp.sum(chosen, axis=1)
    below = jnp.asarray(np.tril(np.ones((row_count, row_count), np.float32), -1), jnp.bfloat16)
    rank = jnp.dot(below, named, preferred_element_type=jnp.float32).astype(jnp.int32)
    per_expert_group = experts // EXPERT_GROUPS
    group_of = jnp.asarray(np.repeat(np.eye(EXPERT_GROUPS, dtype=np.float32), per_expert_group, axis=1))
    group_weight = jnp.sum(expert_group_weight[:, :, None] * group_of[None], axis=1)
    weight = group_weight * jnp.sum(
        chosen.astype(jnp.float32) * chosen_expert_weight[:, :, None], axis=1
    )
    hot = (rank[:, :, None] == jnp.arange(capacity, dtype=jnp.int32)) & (named[:, :, None] > 0)
    pick = hot.astype(jnp.bfloat16).reshape(row_count, experts * capacity)
    route = jnp.where(hot, weight[:, :, None], 0.0).reshape(row_count, experts * capacity)
    route_high = route.astype(jnp.bfloat16)
    route_low = (route - route_high.astype(jnp.float32)).astype(jnp.bfloat16)
    outgoing = lax.dot_general(
        pick, ffn_in, (((0,), (0,)), ((), ())), preferred_element_type=jnp.float32
    ).astype(jnp.bfloat16)
    received = lax.all_to_all(
        outgoing.reshape(experts, capacity, width), ("sp", "tp"), split_axis=0, concat_axis=0,
        tiled=True,
    )
    flat_rows = received.reshape(-1, width)
    gate_part = jnp.dot(flat_rows, expert_gate_weight[0], preferred_element_type=jnp.float32)
    upward = jnp.dot(flat_rows, expert_up_weight[0], preferred_element_type=jnp.float32)
    hidden = (jax.nn.silu(gate_part) * upward).astype(jnp.bfloat16)
    finished = jnp.dot(
        hidden, expert_down_weight[0], preferred_element_type=jnp.float32
    ).astype(jnp.bfloat16)
    returned = lax.all_to_all(
        finished.reshape(received.shape), ("sp", "tp"), split_axis=0, concat_axis=0, tiled=True
    ).reshape(experts * capacity, width)
    summed = (
        mixed_rows.astype(jnp.float32)
        + jnp.dot(route_high, returned, preferred_element_type=jnp.float32)
        + jnp.dot(route_low, returned, preferred_element_type=jnp.float32)
    )
    return summed.astype(jnp.bfloat16)


def solution(mesh):
    placed = (
        P("sp", "tp"),
        P("sp", "tp"),
        P("sp", "tp"),
        P("sp", "tp"),
        P("sp", "tp"),
        P("sp", "tp"),
        P("tp"),
        P("tp"),
        P(None, "tp"),
        P(None, "tp"),
        P(None, "tp"),
        P("sp"),
        P(),
        P(("sp", "tp"), None),
        P(),
        P(),
        P(("sp", "tp"), None),
        P(("sp", "tp"), None),
        P(("sp", "tp"), None),
        P(("sp", "tp"), None, None),
        P(("sp", "tp"), None, None),
        P(("sp", "tp"), None, None),
    )
    return jax.shard_map(
        local, mesh=mesh, in_specs=placed, out_specs=P(("sp", "tp"), None), check_vma=False
    )
```

```python
import functools

import jax
import jax.numpy as jnp
import numpy as np
from jax import lax
from jax.experimental import pallas as pl
from jax.experimental.pallas import tpu as pltpu
from jax.sharding import PartitionSpec as P

D_STATE = 128
EXPERT_GROUPS = 4
LONGEST = 1536
EPSILON = 1e-06

NEG = -1e30
MESH_ID = pl.DeviceIdType.MESH
HOSTS = 4


def softplus(v):
    return jnp.maximum(v, 0.0) + jnp.log1p(jnp.exp(-jnp.abs(v)))


def silu(v):
    return v / (1.0 + jnp.exp(-v))


def exact_dot(a, b):
    return jnp.dot(a, b, preferred_element_type=jnp.float32, precision=lax.Precision.HIGHEST)


def mixer_kernel(
    n, x_hbm, b_hbm, c_hbm, gate_hbm, resid_hbm, w_hbm,
    step_ref, extra_ref, docrow_ref, rate_ref, direct_ref, taps_ref, btaps_ref, ctaps_ref,
    gain_ref, gain2_ref,
    mixed_ref, ffn_ref,
    x_ref, b_ref, c_ref, gate_ref, resid_ref, w_ref, docs_ref, pad, pad_docs,
    edge_x, edge_b, edge_c, edge_d,
    vconv, bconv, cconv, ylocal, cumx, t0, g0, rs, rg, tot, grow, rt, rgrow, hs, incoming,
    gated, regrouped,
    wsem, send, recv,
):
    sp = lax.axis_index("sp")
    tp = lax.axis_index("tp")
    length, channels = x_ref.shape
    state = b_ref.shape[1]
    lanes = 128
    chunks = channels // lanes
    heads = step_ref.shape[0]
    half = length // 2
    edge = edge_x.shape[0]
    hosts, _, block = rs.shape
    member = sp % hosts
    base_sp = sp - member

    loads = [
        pltpu.make_async_copy(source, target, wsem.at[i])
        for i, (source, target) in enumerate((
            (x_hbm, x_ref), (b_hbm, b_ref), (c_hbm, c_ref), (gate_hbm, gate_ref),
            (resid_hbm, resid_ref), (w_hbm, w_ref),
        ))
    ]
    for load in loads:
        load.start()

    docs_row = docrow_ref[...].astype(jnp.float32) + 1.0
    docs_ref[...] = jnp.transpose(jnp.broadcast_to(docs_row, (lanes, length)))

    barrier = pltpu.get_barrier_semaphore()
    count = jnp.int32(hosts)
    pl.semaphore_signal(barrier, inc=1, device_id=(sp, 1 - tp), device_id_type=MESH_ID)
    for d in range(1, hosts):
        pl.semaphore_signal(
            barrier, inc=1, device_id=(base_sp + (member + d) % hosts, tp), device_id_type=MESH_ID
        )
    for off in (1, hosts, 2 * hosts):
        @pl.when(sp + off < n)
        def _():
            pl.semaphore_signal(barrier, inc=1, device_id=(sp + off, tp), device_id_type=MESH_ID)

        @pl.when(sp >= off)
        def _():
            pl.semaphore_signal(barrier, inc=1, device_id=(sp - off, tp), device_id_type=MESH_ID)

        count = count + (sp + off < n).astype(jnp.int32) + (sp >= off).astype(jnp.int32)
    pl.semaphore_wait(barrier, count)

    def remote(sent, received, src, dst, device):
        return pltpu.make_async_remote_copy(
            src_ref=src, dst_ref=dst, send_sem=send.at[sent], recv_sem=recv.at[received],
            device_id=(device, tp), device_id_type=MESH_ID,
        )

    def copy(slot, src, dst, off):
        return remote(slot, slot, src, dst, sp + off)

    def part_of(i):
        return pl.ds(pl.multiple_of(i * block, block), block)

    def give(i, source):
        return [
            remote(4 + i, 4 + source, t0.at[:, part_of(i)], rs.at[source], base_sp + i),
            remote(
                4 + hosts + i, 4 + hosts + source, g0.at[:, part_of(i)], rg.at[source], base_sp + i
            ),
        ]

    def enter(i, source):
        return remote(
            4 + 2 * hosts + i, 4 + 2 * hosts + source, hs.at[i], incoming.at[:, part_of(source)],
            base_sp + i,
        )

    others = [(member + d) % hosts for d in range(1, hosts)]

    last = pl.ds(length - edge, edge)
    edges = [
        copy(0, x_ref.at[last, :], edge_x, 1),
        copy(1, b_ref.at[last, :], edge_b, 1),
        copy(2, c_ref.at[last, :], edge_c, 1),
        copy(3, docs_ref.at[last, :], edge_d, 1),
    ]

    def start(copies, off):
        @pl.when(sp + off < n)
        def _():
            for one in copies:
                one.start()

    def wait_recv(copies, off):
        @pl.when(sp >= off)
        def _():
            for one in copies:
                one.wait_recv()

    def wait_send(copies, off):
        @pl.when(sp + off < n)
        def _():
            for one in copies:
                one.wait_send()

    for load in loads[:3]:
        load.wait()
    start(edges, 1)

    head_row = lax.broadcasted_iota(jnp.int32, (heads, heads), 0)
    head_col = lax.broadcasted_iota(jnp.int32, (heads, heads), 1)

    def column(ref):
        return jnp.sum(jnp.where(head_row == head_col, ref[...], 0.0), axis=1, keepdims=True)

    direct_column = column(direct_ref)
    step = softplus(step_ref[...])
    logs = extra_ref[...] - step * column(rate_ref)
    rows = lax.broadcasted_iota(jnp.int32, (length, length), 0)
    cols = lax.broadcasted_iota(jnp.int32, (length, length), 1)
    causal = rows >= cols
    cum = lax.dot_general(
        causal.astype(jnp.float32), logs, (((1,), (1,)), ((), ())),
        preferred_element_type=jnp.float32, precision=lax.Precision.HIGHEST,
    )
    cum_t = exact_dot(logs, (rows <= cols).astype(jnp.float32))
    same = docs_ref[:, 0:1] == docs_row
    blocked = jnp.where(causal & same, 0.0, NEG)
    tail = (docs_ref[...] == docs_ref[length - 1 : length, :]).astype(jnp.float32)

    pad[edge:, :channels] = x_ref[...].astype(jnp.float32)
    pad[edge:, channels : channels + state] = b_ref[...].astype(jnp.float32)
    pad[edge:, channels + state :] = c_ref[...].astype(jnp.float32)
    pad_docs[edge:, :] = docs_ref[...]

    wait_recv(edges, 1)
    has = sp >= 1
    pad[:edge, :channels] = jnp.where(has, edge_x[...].astype(jnp.float32), 0.0)
    pad[:edge, channels : channels + state] = jnp.where(has, edge_b[...].astype(jnp.float32), 0.0)
    pad[:edge, channels + state :] = jnp.where(has, edge_c[...].astype(jnp.float32), 0.0)
    pad_docs[:edge, :] = jnp.where(has, edge_d[...], 0.0)

    taps_count = taps_ref.shape[0]
    base = edge - taps_count + 1
    masks = [
        (pad_docs[base + k : base + k + length, :] == docs_ref[...]).astype(jnp.float32)
        for k in range(taps_count - 1)
    ]

    def conv(at, taps, start_lane):
        total = taps[taps_count - 1 :, start_lane : start_lane + lanes].astype(
            jnp.float32
        ) * pad[edge : edge + length, at : at + lanes]
        for k in range(taps_count - 1):
            total = total + (
                taps[k : k + 1, start_lane : start_lane + lanes].astype(jnp.float32)
                * pad[base + k : base + k + length, at : at + lanes]
                * masks[k]
            )
        return silu(total).astype(jnp.bfloat16)

    bconv[...] = conv(channels, btaps_ref, 0)
    cconv[...] = conv(channels + state, ctaps_ref, 0)

    keep = (docs_ref[length - 1 : length, :] == pad_docs[edge - 1 : edge, :]).astype(jnp.float32)
    keep = keep * has.astype(jnp.float32)
    b_t = jnp.transpose(bconv[...].astype(jnp.float32)).astype(jnp.bfloat16)
    per_chunk = heads // chunks
    width = lanes // per_chunk
    spread_row = lax.broadcasted_iota(jnp.int32, (heads, lanes), 0) * width
    spread_lane = lax.broadcasted_iota(jnp.int32, (heads, lanes), 1)

    def widen(j):
        at = spread_lane + j * lanes - spread_row
        return jnp.where((at >= 0) & (at < width), 1.0, 0.0)

    for j in range(chunks):
        at = slice(j * lanes, (j + 1) * lanes)
        value = conv(j * lanes, taps_ref, j * lanes)
        vconv[:, at] = value
        wide = widen(j)
        cum_wide = exact_dot(cum, wide)
        cumx[:, at] = cum_wide
        step_wide = lax.dot_general(
            step, wide, (((0,), (0,)), ((), ())),
            preferred_element_type=jnp.float32, precision=lax.Precision.HIGHEST,
        )
        stepped = (step_wide * value.astype(jnp.float32)).astype(jnp.bfloat16)
        ylocal[:, at] = stepped.astype(jnp.float32)
        ending = cum_wide[length - 1 : length, :]
        ended = (jnp.exp(ending - cum_wide) * tail * stepped.astype(jnp.float32)).astype(
            jnp.bfloat16
        )
        t0[:, at] = jnp.dot(b_t, ended, preferred_element_type=jnp.float32).astype(jnp.bfloat16)
        g0[:, at] = jnp.broadcast_to(jnp.exp(ending) * keep, (8, lanes))
        i = j * lanes // block
        if (j + 1) * lanes == (i + 1) * block:
            @pl.when(member != i)
            def _():
                for one in give(i, member):
                    one.start()

            @pl.when(member == i)
            def _():
                rs[i] = t0[:, i * block : (i + 1) * block]
                rg[i] = g0[:, i * block : (i + 1) * block]

    scores = lax.dot_general(
        cconv[...], bconv[...], (((1,), (1,)), ((), ())), preferred_element_type=jnp.float32
    )
    lane = lax.broadcasted_iota(jnp.int32, (length, lanes), 1)

    def inside(j):
        at = slice(j * lanes, (j + 1) * lanes)
        stepped = ylocal[:, at].astype(jnp.bfloat16)
        result = None
        for k in range(per_chunk):
            h = j * per_chunk + k
            decay = jnp.exp(cum[:, h : h + 1] - cum_t[h : h + 1, :] + blocked)
            part = jnp.dot(
                (scores * decay).astype(jnp.bfloat16), stepped, preferred_element_type=jnp.float32
            )
            result = part if result is None else jnp.where(lane < k * width, result, part)
        direct = jnp.sum(widen(j) * direct_column, axis=0, keepdims=True)
        ylocal[:, at] = result + direct * vconv[:, at].astype(jnp.float32)

    early = chunks // 4
    late = chunks * 5 // 8
    for j in range(early):
        inside(j)

    for i in others:
        for one in give(i, i):
            one.wait_recv()
    total = jnp.zeros((state, block), jnp.float32)
    growth = jnp.ones((1, block), jnp.float32)
    for i in range(hosts):
        factor = rg[i][0:1, :]
        total = rs[i].astype(jnp.float32) + factor * total
        growth = growth * factor
    tot[...] = total.astype(jnp.bfloat16)
    grow[...] = jnp.broadcast_to(growth, grow.shape)
    slot = 4 + 3 * hosts
    nearer = [copy(slot, tot, rt.at[0], hosts), copy(slot + 1, grow, rgrow, hosts)]
    further = [copy(slot + 2, tot, rt.at[1], 2 * hosts)]
    start(nearer, hosts)
    start(further, 2 * hosts)
    for j in range(early, late):
        inside(j)

    wait_recv(nearer, hosts)
    wait_recv(further, 2 * hosts)
    carried = jnp.where(sp >= 2 * hosts, rt[1].astype(jnp.float32), 0.0)
    carried = jnp.where(sp >= hosts, rt[0].astype(jnp.float32) + rgrow[0:1, :] * carried, 0.0)
    for i in range(hosts):
        @pl.when(member != i)
        def _():
            hs[i] = carried.astype(jnp.bfloat16)
            enter(i, member).start()

        @pl.when(member == i)
        def _():
            incoming[:, i * block : (i + 1) * block] = carried.astype(jnp.bfloat16)

        if i < hosts - 1:
            carried = rs[i].astype(jnp.float32) + rg[i][0:1, :] * carried
    for j in range(late, chunks):
        inside(j)

    for i in others:
        enter(i, i).wait_recv()
    loads[3].wait()
    entering = (docs_ref[...] == pad_docs[edge - 1 : edge, :]).astype(jnp.float32)
    for j in range(chunks):
        at = slice(j * lanes, (j + 1) * lanes)
        readout = jnp.dot(cconv[...], incoming[:, at], preferred_element_type=jnp.float32)
        whole = ylocal[:, at] + readout * jnp.exp(cumx[:, at]) * entering
        gated[:, at] = (whole * silu(gate_ref[:, at].astype(jnp.float32))).astype(jnp.bfloat16)

    swap = pltpu.make_async_remote_copy(
        src_ref=gated.at[pl.ds(pl.multiple_of((1 - tp) * half, half), half), :],
        dst_ref=regrouped,
        send_sem=send.at[slot + 3], recv_sem=recv.at[slot + 3],
        device_id=(sp, 1 - tp), device_id_type=MESH_ID,
    )
    swap.start()
    wait_send(edges, 1)
    wait_send(nearer, hosts)
    wait_send(further, 2 * hosts)
    for i in others:
        for one in give(i, member):
            one.wait_send()
        enter(i, member).wait_send()
    loads[4].wait()
    loads[5].wait()
    swap.wait()
    own = gated[pl.ds(pl.multiple_of(tp * half, half), half), :].astype(jnp.float32)
    other = regrouped[...].astype(jnp.float32)
    total = jnp.sum(own * own, axis=-1, keepdims=True) + jnp.sum(other * other, axis=-1, keepdims=True)
    features = 2 * channels
    factor = lax.rsqrt(total / features + EPSILON)
    low = jnp.where(tp == 0, own, other)
    high = jnp.where(tp == 0, other, own)
    low = (low * factor * gain_ref[:, :channels]).astype(jnp.bfloat16)
    high = (high * factor * gain_ref[:, channels:]).astype(jnp.bfloat16)
    square = jnp.zeros((half, 1), jnp.float32)
    piece = 512
    model = resid_ref.shape[1]
    for j in range(model // piece):
        at = slice(j * piece, (j + 1) * piece)
        projected = jnp.dot(low, w_ref[:channels, at], preferred_element_type=jnp.float32)
        projected += jnp.dot(high, w_ref[channels:, at], preferred_element_type=jnp.float32)
        mixed = (resid_ref[:, at].astype(jnp.float32) + projected).astype(jnp.bfloat16)
        mixed_ref[:, at] = mixed
        wide = mixed.astype(jnp.float32)
        square += jnp.sum(wide * wide, axis=-1, keepdims=True)
    factor = lax.rsqrt(square / model + EPSILON)
    ffn_ref[...] = (mixed_ref[...].astype(jnp.float32) * factor * gain2_ref[...]).astype(jnp.bfloat16)


def mixer(n, x, b, c, gate, step, extra, rate, direct, taps, btaps, ctaps, docs, gain, resid,
          weight, gain2):
    length, channels = x.shape
    state = b.shape[1]
    half, model = resid.shape
    hosts = HOSTS
    block = channels // hosts
    assert state == D_STATE and n % hosts == 0 and block % 128 == 0
    assert (LONGEST - 2) // (hosts * length) + 1 <= 2
    bf, f32 = jnp.bfloat16, jnp.float32
    edge = 16
    vm = pltpu.VMEM
    sems = 4 + 3 * hosts + 4
    return pl.pallas_call(
        functools.partial(mixer_kernel, n),
        out_shape=[jax.ShapeDtypeStruct((half, model), bf)] * 2,
        in_specs=[pl.BlockSpec(memory_space=pl.ANY)] * 6
        + [pl.BlockSpec(memory_space=pltpu.VMEM)] * 10,
        out_specs=[pl.BlockSpec(memory_space=pltpu.VMEM)] * 2,
        scratch_shapes=[
            vm(x.shape, bf), vm(b.shape, bf), vm(c.shape, bf), vm(gate.shape, bf),
            vm(resid.shape, bf), vm(weight.shape, bf), vm((length, 128), f32),
            vm((edge + length, channels + 2 * state), f32), vm((edge + length, 128), f32),
            vm((edge, channels), bf), vm((edge, state), bf), vm((edge, state), bf),
            vm((edge, 128), f32),
            vm((length, channels), bf), vm((length, state), bf), vm((length, state), bf),
            vm((length, channels), f32), vm((length, channels), f32),
            vm((state, channels), bf), vm((8, channels), f32),
            vm((hosts, state, block), bf), vm((hosts, 8, block), f32),
            vm((state, block), bf), vm((8, block), f32),
            vm((2, state, block), bf), vm((8, block), f32),
            vm((hosts, state, block), bf), vm((state, channels), bf),
            vm((length, channels), bf), vm((half, channels), bf),
            pltpu.SemaphoreType.DMA((6,)), pltpu.SemaphoreType.DMA((sems,)),
            pltpu.SemaphoreType.DMA((sems,)),
        ],
        compiler_params=pltpu.CompilerParams(
            collective_id=0, has_side_effects=True, vmem_limit_bytes=58 * 1024 * 1024
        ),
    )(x, b, c, gate, resid, weight, step.T, extra.T, docs[None, :], rate[None, :], direct[None, :],
      taps, btaps, ctaps, gain[None, :], gain2[None, :])


def plane_kernel(
    planes, tps, ffn_ref, ids_ref, group_ref, weight_ref, mixed_ref, wg_hbm, wu_hbm, wd_hbm,
    out_ref,
    wg, wu, wd, meta, picks, routes, line, slots, arrived, done, back, part, mine, parts,
    wsem, msend, mrecv, lsend, lrecv, fsend, frecv, bsend, brecv, psend, precv,
):
    sp = lax.axis_index("sp")
    tp = lax.axis_index("tp")
    rows, model = ffn_ref.shape
    per = lax.axis_size("sp") * tps // planes
    hosts = per // tps
    cap = rows // per
    experts = planes * per
    chunks = lrecv.shape[1]
    width = model // chunks
    z = sp // hosts
    q = (sp % hosts) * tps + tp

    loads = [
        pltpu.make_async_copy(wg_hbm.at[0], wg, wsem.at[0]),
        pltpu.make_async_copy(wu_hbm.at[0], wu, wsem.at[1]),
        pltpu.make_async_copy(wd_hbm.at[0], wd, wsem.at[2]),
    ]
    for load in loads:
        load.start()

    def place(plane, member):
        return (plane * hosts + member // tps, member % tps)

    def loop(low, high, act):
        def body(k, carry):
            act(k)
            return carry

        lax.fori_loop(low, high, body, 0)

    barrier = pltpu.get_barrier_semaphore()

    def greet(device):
        pl.semaphore_signal(barrier, inc=1, device_id=device, device_id_type=MESH_ID)

    loop(1, per, lambda d: greet(place(z, (q + d) % per)))
    loop(1, planes, lambda d: greet(place((z + d) % planes, q)))

    def columns(c):
        return pl.ds(pl.multiple_of(c * width, width), width)

    def member_rows(member):
        return pl.ds(pl.multiple_of(member * cap, cap), cap)

    def tell(plane, target):
        return pltpu.make_async_remote_copy(
            src_ref=meta.at[plane], dst_ref=meta.at[plane],
            send_sem=msend.at[target], recv_sem=mrecv.at[plane],
            device_id=place(target, q), device_id_type=MESH_ID,
        )

    def hop(plane, c, up):
        return pltpu.make_async_remote_copy(
            src_ref=line.at[plane, :, columns(c)], dst_ref=line.at[plane, :, columns(c)],
            send_sem=lsend.at[up, plane, c], recv_sem=lrecv.at[plane, c],
            device_id=place(z + 2 * up - 1, q), device_id_type=MESH_ID,
        )

    def forward(plane, c, member):
        return pltpu.make_async_remote_copy(
            src_ref=slots.at[plane, member_rows(member), columns(c)],
            dst_ref=arrived.at[plane, member_rows(q), columns(c)],
            send_sem=fsend.at[plane], recv_sem=frecv.at[plane],
            device_id=place(z, member), device_id_type=MESH_ID,
        )

    def backward(plane, c, member):
        return pltpu.make_async_remote_copy(
            src_ref=done.at[plane, member_rows(member), columns(c)],
            dst_ref=back.at[plane, member_rows(q), columns(c)],
            send_sem=bsend.at[plane], recv_sem=brecv.at[plane, c],
            device_id=place(z, member), device_id_type=MESH_ID,
        )

    def home(plane, c):
        return pltpu.make_async_remote_copy(
            src_ref=part.at[plane, :, columns(c)], dst_ref=parts.at[z, :, columns(c)],
            send_sem=psend.at[plane, c], recv_sem=precv.at[z, c],
            device_id=place(plane, q), device_id_type=MESH_ID,
        )

    def homed(plane, c):
        return pltpu.make_async_copy(
            parts.at[plane, :, columns(c)], parts.at[plane, :, columns(c)], precv.at[plane, c]
        )

    others = pl.ds(0, (per - 1) * cap)

    def whole(ref, plane, sem):
        view = ref.at[plane, others, :]
        return pltpu.make_async_copy(view, view, sem.at[plane])

    def slab(plane, c):
        view = back.at[plane, others, columns(c)]
        return pltpu.make_async_copy(view, view, brecv.at[plane, c])

    line[z] = ffn_ref[...]
    ids = ids_ref[...]
    group_size = experts // EXPERT_GROUPS
    weight = jnp.zeros(ids.shape, jnp.float32)
    for g in range(EXPERT_GROUPS):
        inside = (ids >= g * group_size) & (ids < (g + 1) * group_size)
        weight = weight + jnp.where(inside, group_ref[g : g + 1, :], 0.0)
    choose = ids.shape[0]
    info = jnp.concatenate(
        [
            ids.astype(jnp.float32), weight * weight_ref[...],
            jnp.zeros((meta.shape[1] - 2 * choose, rows), jnp.float32),
        ],
        axis=0,
    )
    meta[z] = info
    pl.semaphore_wait(barrier, per + planes - 2)
    loop(1, planes, lambda d: tell(z, (z + d) % planes).start())
    for c in range(chunks):
        @pl.when(z < planes - 1)
        def _():
            hop(z, c, 1).start()

        @pl.when(z > 0)
        def _():
            hop(z, c, 0).start()

    slot_member = lax.broadcasted_iota(jnp.int32, (per, cap, rows), 0).reshape(rows, rows)
    slot_place = lax.broadcasted_iota(jnp.int32, (per, cap, rows), 1).reshape(rows, rows)
    slot_expert = (slot_member + z * per).astype(jnp.float32)
    slot_place = slot_place.astype(jnp.float32)
    earlier = (
        lax.broadcasted_iota(jnp.int32, (rows, rows), 0)
        < lax.broadcasted_iota(jnp.int32, (rows, rows), 1)
    ).astype(jnp.bfloat16)

    def sort_out(plane):
        known = meta[plane]
        named = jnp.zeros((rows, rows), jnp.float32)
        value = jnp.zeros((rows, rows), jnp.float32)
        for k in range(choose):
            chosen = (known[k : k + 1, :] == slot_expert).astype(jnp.float32)
            named = named + chosen
            value = value + chosen * known[choose + k : choose + k + 1, :]
        rank = jnp.dot(named.astype(jnp.bfloat16), earlier, preferred_element_type=jnp.float32)
        hot = jnp.where(rank == slot_place, named, 0.0)
        picks[plane] = hot.astype(jnp.bfloat16)
        routes[plane] = jnp.transpose(hot * value).astype(jnp.bfloat16)

    lag = chunks + 2

    def stage_rows(k, c, up, plane):
        @pl.when(k > 0)
        def _():
            hop(plane, c, up).wait_recv()

            @pl.when((up == 0) & (z < planes - 1))
            def _():
                hop(plane, c, 1).start()

            @pl.when((up == 1) & (z > 0))
            def _():
                hop(plane, c, 0).start()

        @pl.when(c == 0)
        def _():
            @pl.when(k > 0)
            def _():
                tell(plane, plane).wait_recv()

            sort_out(plane)

        at = columns(c)
        slots[plane, :, at] = jnp.dot(
            picks[plane], line[plane, :, at], preferred_element_type=jnp.float32
        ).astype(jnp.bfloat16)
        arrived[plane, member_rows(q), at] = slots[plane, member_rows(q), at]
        loop(1, per, lambda d: forward(plane, c, (q + d) % per).start())

    def stage_experts(k, plane):
        @pl.when(k == 0)
        def _():
            for load in loads:
                load.wait()

        whole(arrived, plane, frecv).wait()
        tokens = arrived[plane]
        gate = jnp.dot(tokens, wg[...], preferred_element_type=jnp.float32)
        up = jnp.dot(tokens, wu[...], preferred_element_type=jnp.float32)
        hidden = (silu(gate) * up).astype(jnp.bfloat16)
        for c in range(chunks):
            at = slice(c * width, (c + 1) * width)
            done[plane, :, at] = jnp.dot(
                hidden, wd[:, at], preferred_element_type=jnp.float32
            ).astype(jnp.bfloat16)
            back[plane, member_rows(q), at] = done[plane, member_rows(q), at]
            loop(1, per, lambda d: backward(plane, c, (q + d) % per).start())

    def stage_home(k, c, plane):
        slab(plane, c).wait()
        at = columns(c)
        total = jnp.dot(
            routes[plane], back[plane, :, at], preferred_element_type=jnp.float32
        )

        @pl.when(k == 0)
        def _():
            mine[:, at] = total

        @pl.when(k > 0)
        def _():
            part[plane, :, at] = total.astype(jnp.bfloat16)
            home(plane, c).start()

    def tick(v):
        def both(k, act):
            def side(up):
                plane = z + k * (2 * up - 1)

                @pl.when((plane >= 0) & (plane < planes) & ((k > 0) | (up == 0)))
                def _():
                    act(up, plane)

            loop(0, 2, side)

        @pl.when(v < planes * chunks)
        def _():
            k = v // chunks
            c = v % chunks
            both(k, lambda up, plane: stage_rows(k, c, up, plane))

        @pl.when((v % chunks == 0) & (v >= chunks) & (v <= planes * chunks))
        def _():
            k = v // chunks - 1
            both(k, lambda up, plane: stage_experts(k, plane))

        @pl.when(v >= lag)
        def _():
            k = (v - lag) // chunks
            c = (v - lag) % chunks
            both(k, lambda up, plane: stage_home(k, c, plane))

    loop(0, planes * chunks + lag, tick)

    for c in range(chunks):
        at = slice(c * width, (c + 1) * width)
        loop(1, planes, lambda d: homed((z + d) % planes, c).wait())
        mine[:, at] = mine[:, at] + mixed_ref[:, at].astype(jnp.float32)

        def add(d):
            mine[:, at] = mine[:, at] + parts[(z + d) % planes, :, at].astype(jnp.float32)

        loop(1, planes, add)
        out_ref[:, at] = mine[:, at].astype(jnp.bfloat16)

    loop(1, planes, lambda d: tell(z, (z + d) % planes).wait_send())

    def finish(plane):
        whole(slots, plane, fsend).wait()
        whole(done, plane, bsend).wait()

        def each(c):
            @pl.when((plane <= z) & (z < planes - 1))
            def _():
                hop(plane, c, 1).wait_send()

            @pl.when((plane >= z) & (z > 0))
            def _():
                hop(plane, c, 0).wait_send()

            @pl.when(plane != z)
            def _():
                home(plane, c).wait_send()

        loop(0, chunks, each)

    loop(0, planes, finish)


def exchange(ffn, ids, group_weight, chosen_weight, mixed, gate_weight, up_weight, down_weight,
             planes):
    rows, model = ffn.shape
    chunks = 4
    bf, f32 = jnp.bfloat16, jnp.float32
    vm = pltpu.VMEM
    dma = pltpu.SemaphoreType.DMA
    return pl.pallas_call(
        functools.partial(plane_kernel, planes, lax.axis_size("tp")),
        out_shape=jax.ShapeDtypeStruct(mixed.shape, bf),
        in_specs=[pl.BlockSpec(memory_space=pltpu.VMEM)] * 5
        + [pl.BlockSpec(memory_space=pl.ANY)] * 3,
        out_specs=pl.BlockSpec(memory_space=pltpu.VMEM),
        scratch_shapes=[
            vm(gate_weight.shape[1:], bf), vm(up_weight.shape[1:], bf),
            vm(down_weight.shape[1:], bf),
            vm((planes, 8, rows), f32),
            vm((planes, rows, rows), bf), vm((planes, rows, rows), bf),
            vm((planes, rows, model), bf), vm((planes, rows, model), bf),
            vm((planes, rows, model), bf), vm((planes, rows, model), bf),
            vm((planes, rows, model), bf), vm((planes, rows, model), bf),
            vm((rows, model), f32), vm((planes, rows, model), bf),
            dma((3,)), dma((planes,)), dma((planes,)),
            dma((2, planes, chunks)), dma((planes, chunks)),
            dma((planes,)), dma((planes,)), dma((planes,)), dma((planes, chunks)),
            dma((planes, chunks)), dma((planes, chunks)),
        ],
        compiler_params=pltpu.CompilerParams(
            collective_id=1, has_side_effects=True, vmem_limit_bytes=56 * 1024 * 1024
        ),
    )(ffn, ids, group_weight, chosen_weight, mixed, gate_weight, up_weight, down_weight)


def local(
    mixer_value_rows,
    input_map_rows,
    output_map_rows,
    gate_preactivation,
    step_preactivation,
    position_extra_decay,
    head_decay_rate,
    head_direct_term,
    value_taps,
    input_map_taps,
    output_map_taps,
    document_index,
    gated_norm_gain,
    residual,
    mixer_output_weight,
    expert_norm_gain,
    expert_group_weight,
    chosen_expert_weight,
    chosen_expert_index,
    expert_gate_weight,
    expert_up_weight,
    expert_down_weight,
):
    mixed_rows, ffn_in = mixer(
        lax.axis_size("sp"), mixer_value_rows, input_map_rows, output_map_rows,
        gate_preactivation, step_preactivation, position_extra_decay, head_decay_rate,
        head_direct_term, value_taps, input_map_taps, output_map_taps, document_index,
        gated_norm_gain, residual, mixer_output_weight, expert_norm_gain,
    )
    experts = lax.axis_size("sp") * lax.axis_size("tp")
    row_count, width = ffn_in.shape
    choose = chosen_expert_index.shape[1]
    capacity = 2 * mixer_value_rows.shape[0] // experts
    per = row_count // capacity
    if (
        capacity % 16 == 0 and row_count % capacity == 0 and experts % per == 0
        and per % lax.axis_size("tp") == 0 and experts % EXPERT_GROUPS == 0 and choose <= 4
    ):
        return exchange(
            ffn_in, chosen_expert_index.T, expert_group_weight.T, chosen_expert_weight.T,
            mixed_rows, expert_gate_weight, expert_up_weight, expert_down_weight, experts // per,
        )
    ids = jnp.arange(experts, dtype=jnp.int32)
    chosen = (chosen_expert_index[:, :, None] == ids).astype(jnp.bfloat16)
    named = jnp.sum(chosen, axis=1)
    below = jnp.asarray(np.tril(np.ones((row_count, row_count), np.float32), -1), jnp.bfloat16)
    rank = jnp.dot(below, named, preferred_element_type=jnp.float32).astype(jnp.int32)
    per_expert_group = experts // EXPERT_GROUPS
    group_of = jnp.asarray(np.repeat(np.eye(EXPERT_GROUPS, dtype=np.float32), per_expert_group, axis=1))
    group_weight = jnp.sum(expert_group_weight[:, :, None] * group_of[None], axis=1)
    weight = group_weight * jnp.sum(
        chosen.astype(jnp.float32) * chosen_expert_weight[:, :, None], axis=1
    )
    hot = (rank[:, :, None] == jnp.arange(capacity, dtype=jnp.int32)) & (named[:, :, None] > 0)
    pick = hot.astype(jnp.bfloat16).reshape(row_count, experts * capacity)
    route = jnp.where(hot, weight[:, :, None], 0.0).reshape(row_count, experts * capacity)
    route_high = route.astype(jnp.bfloat16)
    route_low = (route - route_high.astype(jnp.float32)).astype(jnp.bfloat16)
    outgoing = lax.dot_general(
        pick, ffn_in, (((0,), (0,)), ((), ())), preferred_element_type=jnp.float32
    ).astype(jnp.bfloat16)
    received = lax.all_to_all(
        outgoing.reshape(experts, capacity, width), ("sp", "tp"), split_axis=0, concat_axis=0,
        tiled=True,
    )
    flat_rows = received.reshape(-1, width)
    gate_part = jnp.dot(flat_rows, expert_gate_weight[0], preferred_element_type=jnp.float32)
    upward = jnp.dot(flat_rows, expert_up_weight[0], preferred_element_type=jnp.float32)
    hidden = (jax.nn.silu(gate_part) * upward).astype(jnp.bfloat16)
    finished = jnp.dot(
        hidden, expert_down_weight[0], preferred_element_type=jnp.float32
    ).astype(jnp.bfloat16)
    returned = lax.all_to_all(
        finished.reshape(received.shape), ("sp", "tp"), split_axis=0, concat_axis=0, tiled=True
    ).reshape(experts * capacity, width)
    summed = (
        mixed_rows.astype(jnp.float32)
        + jnp.dot(route_high, returned, preferred_element_type=jnp.float32)
        + jnp.dot(route_low, returned, preferred_element_type=jnp.float32)
    )
    return summed.astype(jnp.bfloat16)


def solution(mesh):
    placed = (
        P("sp", "tp"),
        P("sp", "tp"),
        P("sp", "tp"),
        P("sp", "tp"),
        P("sp", "tp"),
        P("sp", "tp"),
        P("tp"),
        P("tp"),
        P(None, "tp"),
        P(None, "tp"),
        P(None, "tp"),
        P("sp"),
        P(),
        P(("sp", "tp"), None),
        P(),
        P(),
        P(("sp", "tp"), None),
        P(("sp", "tp"), None),
        P(("sp", "tp"), None),
        P(("sp", "tp"), None, None),
        P(("sp", "tp"), None, None),
        P(("sp", "tp"), None, None),
    )
    return jax.shard_map(
        local, mesh=mesh, in_specs=placed, out_specs=P(("sp", "tp"), None), check_vma=False
    )
```

```python
import functools

import jax
import jax.numpy as jnp
import numpy as np
from jax import lax
from jax.experimental import pallas as pl
from jax.experimental.pallas import tpu as pltpu
from jax.sharding import PartitionSpec as P

D_STATE = 128
EXPERT_GROUPS = 4
LONGEST = 1536
EPSILON = 1e-06

NEG = -1e30
MESH_ID = pl.DeviceIdType.MESH
HOSTS = 4


def softplus(v):
    return jnp.maximum(v, 0.0) + jnp.log1p(jnp.exp(-jnp.abs(v)))


def silu(v):
    return v / (1.0 + jnp.exp(-v))


def exact_dot(a, b):
    return jnp.dot(a, b, preferred_element_type=jnp.float32, precision=lax.Precision.HIGHEST)


def mixer_kernel(
    n, greet, begin, x_hbm, b_hbm, c_hbm, gate_hbm, resid_hbm, w_hbm,
    step_ref, extra_ref, docrow_ref, rate_ref, direct_ref, taps_ref, btaps_ref, ctaps_ref,
    gain_ref, gain2_ref,
    mixed_ref, ffn_ref,
    x_ref, b_ref, c_ref, gate_ref, resid_ref, w_ref, docs_ref, pad, pad_docs,
    edge_x, edge_b, edge_c, edge_d,
    vconv, bconv, cconv, ylocal, cumx, t0, g0, rs, rg, tot, grow, rt, rgrow, hs, incoming,
    gated, regrouped,
    wsem, send, recv,
):
    sp = lax.axis_index("sp")
    tp = lax.axis_index("tp")
    length, channels = x_ref.shape
    state = b_ref.shape[1]
    lanes = 128
    chunks = channels // lanes
    heads = step_ref.shape[0]
    half = length // 2
    edge = edge_x.shape[0]
    hosts, _, block = rs.shape
    member = sp % hosts
    base_sp = sp - member

    loads = [
        pltpu.make_async_copy(source, target, wsem.at[i])
        for i, (source, target) in enumerate((
            (x_hbm, x_ref), (b_hbm, b_ref), (c_hbm, c_ref), (gate_hbm, gate_ref),
            (resid_hbm, resid_ref), (w_hbm, w_ref),
        ))
    ]
    for load in loads:
        load.start()

    docs_row = docrow_ref[...].astype(jnp.float32) + 1.0
    docs_ref[...] = jnp.transpose(jnp.broadcast_to(docs_row, (lanes, length)))

    barrier = pltpu.get_barrier_semaphore()
    count = jnp.int32(hosts)
    pl.semaphore_signal(barrier, inc=1, device_id=(sp, 1 - tp), device_id_type=MESH_ID)
    for d in range(1, hosts):
        pl.semaphore_signal(
            barrier, inc=1, device_id=(base_sp + (member + d) % hosts, tp), device_id_type=MESH_ID
        )
    for off in (1, hosts, 2 * hosts):
        @pl.when(sp + off < n)
        def _():
            pl.semaphore_signal(barrier, inc=1, device_id=(sp + off, tp), device_id_type=MESH_ID)

        @pl.when(sp >= off)
        def _():
            pl.semaphore_signal(barrier, inc=1, device_id=(sp - off, tp), device_id_type=MESH_ID)

        count = count + (sp + off < n).astype(jnp.int32) + (sp >= off).astype(jnp.int32)
    if greet is not None:
        count = count + greet(barrier)
    pl.semaphore_wait(barrier, count)

    def remote(sent, received, src, dst, device):
        return pltpu.make_async_remote_copy(
            src_ref=src, dst_ref=dst, send_sem=send.at[sent], recv_sem=recv.at[received],
            device_id=(device, tp), device_id_type=MESH_ID,
        )

    def copy(slot, src, dst, off):
        return remote(slot, slot, src, dst, sp + off)

    def part_of(i):
        return pl.ds(pl.multiple_of(i * block, block), block)

    def give(i, source):
        return [
            remote(4 + i, 4 + source, t0.at[:, part_of(i)], rs.at[source], base_sp + i),
            remote(
                4 + hosts + i, 4 + hosts + source, g0.at[:, part_of(i)], rg.at[source], base_sp + i
            ),
        ]

    def enter(i, source):
        return remote(
            4 + 2 * hosts + i, 4 + 2 * hosts + source, hs.at[i], incoming.at[:, part_of(source)],
            base_sp + i,
        )

    others = [(member + d) % hosts for d in range(1, hosts)]

    last = pl.ds(length - edge, edge)
    edges = [
        copy(0, x_ref.at[last, :], edge_x, 1),
        copy(1, b_ref.at[last, :], edge_b, 1),
        copy(2, c_ref.at[last, :], edge_c, 1),
        copy(3, docs_ref.at[last, :], edge_d, 1),
    ]

    def start(copies, off):
        @pl.when(sp + off < n)
        def _():
            for one in copies:
                one.start()

    def wait_recv(copies, off):
        @pl.when(sp >= off)
        def _():
            for one in copies:
                one.wait_recv()

    def wait_send(copies, off):
        @pl.when(sp + off < n)
        def _():
            for one in copies:
                one.wait_send()

    for load in loads[:3]:
        load.wait()
    start(edges, 1)
    if begin is not None:
        begin()

    head_row = lax.broadcasted_iota(jnp.int32, (heads, heads), 0)
    head_col = lax.broadcasted_iota(jnp.int32, (heads, heads), 1)

    def column(ref):
        return jnp.sum(jnp.where(head_row == head_col, ref[...], 0.0), axis=1, keepdims=True)

    direct_column = column(direct_ref)
    step = softplus(step_ref[...])
    logs = extra_ref[...] - step * column(rate_ref)
    rows = lax.broadcasted_iota(jnp.int32, (length, length), 0)
    cols = lax.broadcasted_iota(jnp.int32, (length, length), 1)
    causal = rows >= cols
    cum = lax.dot_general(
        causal.astype(jnp.float32), logs, (((1,), (1,)), ((), ())),
        preferred_element_type=jnp.float32, precision=lax.Precision.HIGHEST,
    )
    cum_t = exact_dot(logs, (rows <= cols).astype(jnp.float32))
    same = docs_ref[:, 0:1] == docs_row
    blocked = jnp.where(causal & same, 0.0, NEG)
    tail = (docs_ref[...] == docs_ref[length - 1 : length, :]).astype(jnp.float32)

    pad[edge:, :channels] = x_ref[...].astype(jnp.float32)
    pad[edge:, channels : channels + state] = b_ref[...].astype(jnp.float32)
    pad[edge:, channels + state :] = c_ref[...].astype(jnp.float32)
    pad_docs[edge:, :] = docs_ref[...]

    wait_recv(edges, 1)
    has = sp >= 1
    pad[:edge, :channels] = jnp.where(has, edge_x[...].astype(jnp.float32), 0.0)
    pad[:edge, channels : channels + state] = jnp.where(has, edge_b[...].astype(jnp.float32), 0.0)
    pad[:edge, channels + state :] = jnp.where(has, edge_c[...].astype(jnp.float32), 0.0)
    pad_docs[:edge, :] = jnp.where(has, edge_d[...], 0.0)

    taps_count = taps_ref.shape[0]
    base = edge - taps_count + 1
    masks = [
        (pad_docs[base + k : base + k + length, :] == docs_ref[...]).astype(jnp.float32)
        for k in range(taps_count - 1)
    ]

    def conv(at, taps, start_lane):
        total = taps[taps_count - 1 :, start_lane : start_lane + lanes].astype(
            jnp.float32
        ) * pad[edge : edge + length, at : at + lanes]
        for k in range(taps_count - 1):
            total = total + (
                taps[k : k + 1, start_lane : start_lane + lanes].astype(jnp.float32)
                * pad[base + k : base + k + length, at : at + lanes]
                * masks[k]
            )
        return silu(total).astype(jnp.bfloat16)

    bconv[...] = conv(channels, btaps_ref, 0)
    cconv[...] = conv(channels + state, ctaps_ref, 0)

    keep = (docs_ref[length - 1 : length, :] == pad_docs[edge - 1 : edge, :]).astype(jnp.float32)
    keep = keep * has.astype(jnp.float32)
    b_t = jnp.transpose(bconv[...].astype(jnp.float32)).astype(jnp.bfloat16)
    per_chunk = heads // chunks
    width = lanes // per_chunk
    spread_row = lax.broadcasted_iota(jnp.int32, (heads, lanes), 0) * width
    spread_lane = lax.broadcasted_iota(jnp.int32, (heads, lanes), 1)

    def widen(j):
        at = spread_lane + j * lanes - spread_row
        return jnp.where((at >= 0) & (at < width), 1.0, 0.0)

    for j in range(chunks):
        at = slice(j * lanes, (j + 1) * lanes)
        value = conv(j * lanes, taps_ref, j * lanes)
        vconv[:, at] = value
        wide = widen(j)
        cum_wide = exact_dot(cum, wide)
        cumx[:, at] = cum_wide
        step_wide = lax.dot_general(
            step, wide, (((0,), (0,)), ((), ())),
            preferred_element_type=jnp.float32, precision=lax.Precision.HIGHEST,
        )
        stepped = (step_wide * value.astype(jnp.float32)).astype(jnp.bfloat16)
        ylocal[:, at] = stepped.astype(jnp.float32)
        ending = cum_wide[length - 1 : length, :]
        ended = (jnp.exp(ending - cum_wide) * tail * stepped.astype(jnp.float32)).astype(
            jnp.bfloat16
        )
        t0[:, at] = jnp.dot(b_t, ended, preferred_element_type=jnp.float32).astype(jnp.bfloat16)
        g0[:, at] = jnp.broadcast_to(jnp.exp(ending) * keep, (8, lanes))
        i = j * lanes // block
        if (j + 1) * lanes == (i + 1) * block:
            @pl.when(member != i)
            def _():
                for one in give(i, member):
                    one.start()

            @pl.when(member == i)
            def _():
                rs[i] = t0[:, i * block : (i + 1) * block]
                rg[i] = g0[:, i * block : (i + 1) * block]

    scores = lax.dot_general(
        cconv[...], bconv[...], (((1,), (1,)), ((), ())), preferred_element_type=jnp.float32
    )
    lane = lax.broadcasted_iota(jnp.int32, (length, lanes), 1)

    def inside(j):
        at = slice(j * lanes, (j + 1) * lanes)
        stepped = ylocal[:, at].astype(jnp.bfloat16)
        result = None
        for k in range(per_chunk):
            h = j * per_chunk + k
            decay = jnp.exp(cum[:, h : h + 1] - cum_t[h : h + 1, :] + blocked)
            part = jnp.dot(
                (scores * decay).astype(jnp.bfloat16), stepped, preferred_element_type=jnp.float32
            )
            result = part if result is None else jnp.where(lane < k * width, result, part)
        direct = jnp.sum(widen(j) * direct_column, axis=0, keepdims=True)
        ylocal[:, at] = result + direct * vconv[:, at].astype(jnp.float32)

    early = chunks // 4
    late = chunks * 5 // 8
    for j in range(early):
        inside(j)

    for i in others:
        for one in give(i, i):
            one.wait_recv()
    total = jnp.zeros((state, block), jnp.float32)
    growth = jnp.ones((1, block), jnp.float32)
    for i in range(hosts):
        factor = rg[i][0:1, :]
        total = rs[i].astype(jnp.float32) + factor * total
        growth = growth * factor
    tot[...] = total.astype(jnp.bfloat16)
    grow[...] = jnp.broadcast_to(growth, grow.shape)
    slot = 4 + 3 * hosts
    nearer = [copy(slot, tot, rt.at[0], hosts), copy(slot + 1, grow, rgrow, hosts)]
    further = [copy(slot + 2, tot, rt.at[1], 2 * hosts)]
    start(nearer, hosts)
    start(further, 2 * hosts)
    for j in range(early, late):
        inside(j)

    wait_recv(nearer, hosts)
    wait_recv(further, 2 * hosts)
    carried = jnp.where(sp >= 2 * hosts, rt[1].astype(jnp.float32), 0.0)
    carried = jnp.where(sp >= hosts, rt[0].astype(jnp.float32) + rgrow[0:1, :] * carried, 0.0)
    for i in range(hosts):
        @pl.when(member != i)
        def _():
            hs[i] = carried.astype(jnp.bfloat16)
            enter(i, member).start()

        @pl.when(member == i)
        def _():
            incoming[:, i * block : (i + 1) * block] = carried.astype(jnp.bfloat16)

        if i < hosts - 1:
            carried = rs[i].astype(jnp.float32) + rg[i][0:1, :] * carried
    for j in range(late, chunks):
        inside(j)

    for i in others:
        enter(i, i).wait_recv()
    loads[3].wait()
    entering = (docs_ref[...] == pad_docs[edge - 1 : edge, :]).astype(jnp.float32)
    for j in range(chunks):
        at = slice(j * lanes, (j + 1) * lanes)
        readout = jnp.dot(cconv[...], incoming[:, at], preferred_element_type=jnp.float32)
        whole = ylocal[:, at] + readout * jnp.exp(cumx[:, at]) * entering
        gated[:, at] = (whole * silu(gate_ref[:, at].astype(jnp.float32))).astype(jnp.bfloat16)

    swap = pltpu.make_async_remote_copy(
        src_ref=gated.at[pl.ds(pl.multiple_of((1 - tp) * half, half), half), :],
        dst_ref=regrouped,
        send_sem=send.at[slot + 3], recv_sem=recv.at[slot + 3],
        device_id=(sp, 1 - tp), device_id_type=MESH_ID,
    )
    swap.start()
    wait_send(edges, 1)
    wait_send(nearer, hosts)
    wait_send(further, 2 * hosts)
    for i in others:
        for one in give(i, member):
            one.wait_send()
        enter(i, member).wait_send()
    loads[4].wait()
    loads[5].wait()
    swap.wait()
    own = gated[pl.ds(pl.multiple_of(tp * half, half), half), :].astype(jnp.float32)
    other = regrouped[...].astype(jnp.float32)
    total = jnp.sum(own * own, axis=-1, keepdims=True) + jnp.sum(other * other, axis=-1, keepdims=True)
    features = 2 * channels
    factor = lax.rsqrt(total / features + EPSILON)
    low = jnp.where(tp == 0, own, other)
    high = jnp.where(tp == 0, other, own)
    low = (low * factor * gain_ref[:, :channels]).astype(jnp.bfloat16)
    high = (high * factor * gain_ref[:, channels:]).astype(jnp.bfloat16)
    square = jnp.zeros((half, 1), jnp.float32)
    piece = 512
    model = resid_ref.shape[1]
    for j in range(model // piece):
        at = slice(j * piece, (j + 1) * piece)
        projected = jnp.dot(low, w_ref[:channels, at], preferred_element_type=jnp.float32)
        projected += jnp.dot(high, w_ref[channels:, at], preferred_element_type=jnp.float32)
        mixed = (resid_ref[:, at].astype(jnp.float32) + projected).astype(jnp.bfloat16)
        mixed_ref[:, at] = mixed
        wide = mixed.astype(jnp.float32)
        square += jnp.sum(wide * wide, axis=-1, keepdims=True)
    factor = lax.rsqrt(square / model + EPSILON)
    ffn_ref[...] = (mixed_ref[...].astype(jnp.float32) * factor * gain2_ref[...]).astype(jnp.bfloat16)


def mixer_operands(x, b, c, gate, step, extra, rate, direct, taps, btaps, ctaps, docs, gain, resid,
                   weight, gain2):
    return (x, b, c, gate, resid, weight), (
        step.T, extra.T, docs[None, :], rate[None, :], direct[None, :], taps, btaps, ctaps,
        gain[None, :], gain2[None, :],
    )


def mixer_scratch(n, x, b, c, gate, resid, weight):
    length, channels = x.shape
    state = b.shape[1]
    half = resid.shape[0]
    hosts = HOSTS
    block = channels // hosts
    assert state == D_STATE and n % hosts == 0 and block % 128 == 0
    assert (LONGEST - 2) // (hosts * length) + 1 <= 2
    bf, f32 = jnp.bfloat16, jnp.float32
    edge = 16
    vm = pltpu.VMEM
    sems = 4 + 3 * hosts + 4
    return [
        vm(x.shape, bf), vm(b.shape, bf), vm(c.shape, bf), vm(gate.shape, bf),
        vm(resid.shape, bf), vm(weight.shape, bf), vm((length, 128), f32),
        vm((edge + length, channels + 2 * state), f32), vm((edge + length, 128), f32),
        vm((edge, channels), bf), vm((edge, state), bf), vm((edge, state), bf),
        vm((edge, 128), f32),
        vm((length, channels), bf), vm((length, state), bf), vm((length, state), bf),
        vm((length, channels), f32), vm((length, channels), f32),
        vm((state, channels), bf), vm((8, channels), f32),
        vm((hosts, state, block), bf), vm((hosts, 8, block), f32),
        vm((state, block), bf), vm((8, block), f32),
        vm((2, state, block), bf), vm((8, block), f32),
        vm((hosts, state, block), bf), vm((state, channels), bf),
        vm((length, channels), bf), vm((half, channels), bf),
        pltpu.SemaphoreType.DMA((6,)), pltpu.SemaphoreType.DMA((sems,)),
        pltpu.SemaphoreType.DMA((sems,)),
    ]


def mixer(n, operands):
    large, small = mixer_operands(*operands)
    return pl.pallas_call(
        functools.partial(mixer_kernel, n, None, None),
        out_shape=[jax.ShapeDtypeStruct(large[4].shape, jnp.bfloat16)] * 2,
        in_specs=[pl.BlockSpec(memory_space=pl.ANY)] * len(large)
        + [pl.BlockSpec(memory_space=pltpu.VMEM)] * len(small),
        out_specs=[pl.BlockSpec(memory_space=pltpu.VMEM)] * 2,
        scratch_shapes=mixer_scratch(n, *large),
        compiler_params=pltpu.CompilerParams(
            collective_id=0, has_side_effects=True, vmem_limit_bytes=58 * 1024 * 1024
        ),
    )(*large, *small)


def layer_kernel(planes, tps, large, small, *refs):
    mixer_in = refs[: large + small]
    refs = refs[large + small :]
    ids_ref, group_ref, weight_ref, wg_hbm, wu_hbm, wd_hbm, out_ref = refs[:7]
    (
        mixed_ref, wg, wu, wd, meta, picks, routes, line, slots, arrived, done, back, part, mine,
        parts,
        wsem, msend, mrecv, lsend, lrecv, fsend, frecv, bsend, brecv, psend, precv,
    ) = refs[7:33]
    mixer_scratch_refs = refs[33:]
    sp = lax.axis_index("sp")
    tp = lax.axis_index("tp")
    rows, model = mixed_ref.shape
    per = lax.axis_size("sp") * tps // planes
    hosts = per // tps
    cap = rows // per
    experts = planes * per
    chunks = lrecv.shape[1]
    width = model // chunks
    z = sp // hosts
    q = (sp % hosts) * tps + tp

    loads = [
        pltpu.make_async_copy(wg_hbm.at[0], wg, wsem.at[0]),
        pltpu.make_async_copy(wu_hbm.at[0], wu, wsem.at[1]),
        pltpu.make_async_copy(wd_hbm.at[0], wd, wsem.at[2]),
    ]

    def place(plane, member):
        return (plane * hosts + member // tps, member % tps)

    def loop(low, high, act):
        def body(k, carry):
            act(k)
            return carry

        lax.fori_loop(low, high, body, 0)

    def greet(barrier):
        def signal(device):
            pl.semaphore_signal(barrier, inc=1, device_id=device, device_id_type=MESH_ID)

        loop(1, per, lambda d: signal(place(z, (q + d) % per)))
        loop(1, planes, lambda d: signal(place((z + d) % planes, q)))
        return per + planes - 2

    def columns(c):
        return pl.ds(pl.multiple_of(c * width, width), width)

    def member_rows(member):
        return pl.ds(pl.multiple_of(member * cap, cap), cap)

    def tell(plane, target):
        return pltpu.make_async_remote_copy(
            src_ref=meta.at[plane], dst_ref=meta.at[plane],
            send_sem=msend.at[target], recv_sem=mrecv.at[plane],
            device_id=place(target, q), device_id_type=MESH_ID,
        )

    def hop(plane, c, up):
        return pltpu.make_async_remote_copy(
            src_ref=line.at[plane, :, columns(c)], dst_ref=line.at[plane, :, columns(c)],
            send_sem=lsend.at[up, plane, c], recv_sem=lrecv.at[plane, c],
            device_id=place(z + 2 * up - 1, q), device_id_type=MESH_ID,
        )

    peers = [
        ((q + d) % per, place(z, (q + d) % per)) for d in range(1, per)
    ]

    def forward(plane, c, peer):
        member, device = peer
        return pltpu.make_async_remote_copy(
            src_ref=slots.at[plane, member_rows(member), columns(c)],
            dst_ref=arrived.at[plane, member_rows(q), columns(c)],
            send_sem=fsend.at[plane], recv_sem=frecv.at[plane],
            device_id=device, device_id_type=MESH_ID,
        )

    def backward(plane, c, peer):
        member, device = peer
        return pltpu.make_async_remote_copy(
            src_ref=done.at[plane, member_rows(member), columns(c)],
            dst_ref=back.at[plane, member_rows(q), columns(c)],
            send_sem=bsend.at[plane], recv_sem=brecv.at[plane, c],
            device_id=device, device_id_type=MESH_ID,
        )

    def home(plane, c, up):
        landing = jnp.where((up == 0) & (plane == z - 1), planes, plane)
        return pltpu.make_async_remote_copy(
            src_ref=part.at[plane, :, columns(c)], dst_ref=parts.at[landing, :, columns(c)],
            send_sem=psend.at[plane, c], recv_sem=precv.at[landing, c],
            device_id=place(z + 2 * up - 1, q), device_id_type=MESH_ID,
        )

    def homed(landing, c):
        view = parts.at[landing, :, columns(c)]
        return pltpu.make_async_copy(view, view, precv.at[landing, c])

    others = pl.ds(0, (per - 1) * cap)

    def whole(ref, plane, sem):
        view = ref.at[plane, others, :]
        return pltpu.make_async_copy(view, view, sem.at[plane])

    def slab(plane, c):
        view = back.at[plane, others, columns(c)]
        return pltpu.make_async_copy(view, view, brecv.at[plane, c])

    choose = ids_ref.shape[0]

    def begin():
        for load in loads:
            load.start()
        ids = ids_ref[...]
        group_size = experts // EXPERT_GROUPS
        weight = jnp.zeros(ids.shape, jnp.float32)
        for g in range(EXPERT_GROUPS):
            inside = (ids >= g * group_size) & (ids < (g + 1) * group_size)
            weight = weight + jnp.where(inside, group_ref[g : g + 1, :], 0.0)
        meta[z] = jnp.concatenate(
            [
                ids.astype(jnp.float32), weight * weight_ref[...],
                jnp.zeros((meta.shape[1] - 2 * choose, rows), jnp.float32),
            ],
            axis=0,
        )
        loop(1, planes, lambda d: tell(z, (z + d) % planes).start())

    mixer_kernel(
        lax.axis_size("sp"), greet, begin, *mixer_in, mixed_ref, line.at[z], *mixer_scratch_refs
    )
    for c in range(chunks):
        @pl.when(z < planes - 1)
        def _():
            hop(z, c, 1).start()

        @pl.when(z > 0)
        def _():
            hop(z, c, 0).start()

    slot_member = lax.broadcasted_iota(jnp.int32, (per, cap, rows), 0).reshape(rows, rows)
    slot_place = lax.broadcasted_iota(jnp.int32, (per, cap, rows), 1).reshape(rows, rows)
    slot_expert = (slot_member + z * per).astype(jnp.float32)
    slot_place = slot_place.astype(jnp.float32)
    earlier = (
        lax.broadcasted_iota(jnp.int32, (rows, rows), 0)
        < lax.broadcasted_iota(jnp.int32, (rows, rows), 1)
    ).astype(jnp.bfloat16)

    def sort_out(plane):
        known = meta[plane]
        named = jnp.zeros((rows, rows), jnp.float32)
        value = jnp.zeros((rows, rows), jnp.float32)
        for k in range(choose):
            chosen = (known[k : k + 1, :] == slot_expert).astype(jnp.float32)
            named = named + chosen
            value = value + chosen * known[choose + k : choose + k + 1, :]
        rank = jnp.dot(named.astype(jnp.bfloat16), earlier, preferred_element_type=jnp.float32)
        hot = jnp.where(rank == slot_place, named, 0.0)
        picks[plane] = hot.astype(jnp.bfloat16)
        routes[plane] = jnp.transpose(hot * value).astype(jnp.bfloat16)

    lag = chunks + 2

    def stage_rows(k, c, up, plane):
        @pl.when(k > 0)
        def _():
            hop(plane, c, up).wait_recv()

            @pl.when((up == 0) & (z < planes - 1))
            def _():
                hop(plane, c, 1).start()

            @pl.when((up == 1) & (z > 0))
            def _():
                hop(plane, c, 0).start()

        @pl.when(c == 0)
        def _():
            @pl.when(k > 0)
            def _():
                tell(plane, plane).wait_recv()

            sort_out(plane)

        at = columns(c)
        slots[plane, :, at] = jnp.dot(
            picks[plane], line[plane, :, at], preferred_element_type=jnp.float32
        ).astype(jnp.bfloat16)
        arrived[plane, member_rows(q), at] = slots[plane, member_rows(q), at]
        for peer in peers:
            forward(plane, c, peer).start()

    def stage_experts(k, plane):
        @pl.when(k == 0)
        def _():
            for load in loads:
                load.wait()

        whole(arrived, plane, frecv).wait()
        tokens = arrived[plane]
        gate = jnp.dot(tokens, wg[...], preferred_element_type=jnp.float32)
        up = jnp.dot(tokens, wu[...], preferred_element_type=jnp.float32)
        hidden = (silu(gate) * up).astype(jnp.bfloat16)
        for c in range(chunks):
            at = slice(c * width, (c + 1) * width)
            done[plane, :, at] = jnp.dot(
                hidden, wd[:, at], preferred_element_type=jnp.float32
            ).astype(jnp.bfloat16)
            back[plane, member_rows(q), at] = done[plane, member_rows(q), at]
            for peer in peers:
                backward(plane, c, peer).start()

    def stage_home(k, c, plane):
        slab(plane, c).wait()
        at = columns(c)
        total = jnp.dot(
            routes[plane], back[plane, :, at], preferred_element_type=jnp.float32
        )

        @pl.when(k == 0)
        def _():
            mine[:, at] = total

        @pl.when(k > 0)
        def _():
            part[plane, :, at] = total.astype(jnp.bfloat16)

        @pl.when((z == 0) & (k > 0))
        def _():
            home(plane, c, 1).start()

        @pl.when((z == planes - 1) & (k > 0))
        def _():
            home(plane, c, 0).start()

    def tick(v):
        def both(k, act):
            def side(up):
                plane = z + k * (2 * up - 1)

                @pl.when((plane >= 0) & (plane < planes) & ((k > 0) | (up == 0)))
                def _():
                    act(up, plane)

            loop(0, 2, side)

        @pl.when(v < planes * chunks)
        def _():
            k = v // chunks
            c = v % chunks
            both(k, lambda up, plane: stage_rows(k, c, up, plane))

        @pl.when((v % chunks == 0) & (v >= chunks) & (v <= planes * chunks))
        def _():
            k = v // chunks - 1
            both(k, lambda up, plane: stage_experts(k, plane))

        @pl.when(v >= lag)
        def _():
            k = (v - lag) // chunks
            c = (v - lag) % chunks
            both(k, lambda up, plane: stage_home(k, c, plane))

    loop(0, planes * chunks + lag, tick)

    def pass_on(plane, c, up):
        at = columns(c)
        homed(plane, c).wait()
        part[plane, :, at] = (
            part[plane, :, at].astype(jnp.float32) + parts[plane, :, at].astype(jnp.float32)
        ).astype(jnp.bfloat16)
        home(plane, c, up).start()

    behind = 1

    def relay(v):
        def serve(w, up):
            reach = 1 + w // chunks
            plane = jnp.where(up == 1, reach, planes - 1 - reach)
            valid = jnp.where(up == 1, (plane > z) & (z > 0), (plane < z) & (z < planes - 1))

            @pl.when(valid & (w >= 0) & (w < (planes - 1) * chunks))
            def _():
                pass_on(plane, w % chunks, up)

        leading = jnp.where(2 * z < planes, 1, 0)
        loop(0, 2, lambda i: serve(v - i * behind, jnp.where(i == 0, leading, 1 - leading)))

    loop(0, (planes - 1) * chunks + behind, relay)

    for c in range(chunks):
        at = slice(c * width, (c + 1) * width)
        mine[:, at] = mine[:, at] + mixed_ref[:, at].astype(jnp.float32)

        def add(landing):
            homed(landing, c).wait()
            mine[:, at] = mine[:, at] + parts[landing, :, at].astype(jnp.float32)

        @pl.when(z > 0)
        def _():
            add(z)

        @pl.when(z < planes - 1)
        def _():
            add(planes)

        out_ref[:, at] = mine[:, at].astype(jnp.bfloat16)

    loop(1, planes, lambda d: tell(z, (z + d) % planes).wait_send())

    def finish(plane):
        whole(slots, plane, fsend).wait()
        whole(done, plane, bsend).wait()

        def each(c):
            @pl.when((plane <= z) & (z < planes - 1))
            def _():
                hop(plane, c, 1).wait_send()

            @pl.when((plane >= z) & (z > 0))
            def _():
                hop(plane, c, 0).wait_send()

            @pl.when(plane != z)
            def _():
                home(plane, c, 1).wait_send()

        loop(0, chunks, each)

    loop(0, planes, finish)


def layer(n, operands, ids, group_weight, chosen_weight, gate_weight, up_weight, down_weight,
          planes):
    large, small = mixer_operands(*operands)
    rows, model = large[4].shape
    chunks = 4
    bf, f32 = jnp.bfloat16, jnp.float32
    vm = pltpu.VMEM
    dma = pltpu.SemaphoreType.DMA
    return pl.pallas_call(
        functools.partial(layer_kernel, planes, lax.axis_size("tp"), len(large), len(small)),
        out_shape=jax.ShapeDtypeStruct((rows, model), bf),
        in_specs=[pl.BlockSpec(memory_space=pl.ANY)] * len(large)
        + [pl.BlockSpec(memory_space=pltpu.VMEM)] * (len(small) + 3)
        + [pl.BlockSpec(memory_space=pl.ANY)] * 3,
        out_specs=pl.BlockSpec(memory_space=pltpu.VMEM),
        scratch_shapes=[
            vm((rows, model), bf),
            vm(gate_weight.shape[1:], bf), vm(up_weight.shape[1:], bf),
            vm(down_weight.shape[1:], bf),
            vm((planes, 8, rows), f32),
            vm((planes, rows, rows), bf), vm((planes, rows, rows), bf),
            vm((planes, rows, model), bf), vm((planes, rows, model), bf),
            vm((planes, rows, model), bf), vm((planes, rows, model), bf),
            vm((planes, rows, model), bf), vm((planes, rows, model), bf),
            vm((rows, model), f32), vm((planes + 1, rows, model), bf),
            dma((3,)), dma((planes,)), dma((planes,)),
            dma((2, planes, chunks)), dma((planes, chunks)),
            dma((planes,)), dma((planes,)), dma((planes,)), dma((planes, chunks)),
            dma((planes, chunks)), dma((planes + 1, chunks)),
        ] + mixer_scratch(n, *large),
        compiler_params=pltpu.CompilerParams(
            collective_id=1, has_side_effects=True, vmem_limit_bytes=62 * 1024 * 1024
        ),
    )(*large, *small, ids, group_weight, chosen_weight, gate_weight, up_weight, down_weight)


def local(
    mixer_value_rows,
    input_map_rows,
    output_map_rows,
    gate_preactivation,
    step_preactivation,
    position_extra_decay,
    head_decay_rate,
    head_direct_term,
    value_taps,
    input_map_taps,
    output_map_taps,
    document_index,
    gated_norm_gain,
    residual,
    mixer_output_weight,
    expert_norm_gain,
    expert_group_weight,
    chosen_expert_weight,
    chosen_expert_index,
    expert_gate_weight,
    expert_up_weight,
    expert_down_weight,
):
    operands = (
        mixer_value_rows, input_map_rows, output_map_rows, gate_preactivation, step_preactivation,
        position_extra_decay, head_decay_rate, head_direct_term, value_taps, input_map_taps,
        output_map_taps, document_index, gated_norm_gain, residual, mixer_output_weight,
        expert_norm_gain,
    )
    hosts, tps = lax.axis_size("sp"), lax.axis_size("tp")
    experts = hosts * tps
    row_count, width = residual.shape
    choose = chosen_expert_index.shape[1]
    capacity = 2 * mixer_value_rows.shape[0] // experts
    per = row_count // capacity
    if (
        capacity % 16 == 0 and row_count % capacity == 0 and experts % per == 0
        and per % tps == 0 and experts % EXPERT_GROUPS == 0 and choose <= 4 and experts >= 2 * per
    ):
        return layer(
            hosts, operands, chosen_expert_index.T, expert_group_weight.T, chosen_expert_weight.T,
            expert_gate_weight, expert_up_weight, expert_down_weight, experts // per,
        )
    mixed_rows, ffn_in = mixer(hosts, operands)
    ids = jnp.arange(experts, dtype=jnp.int32)
    chosen = (chosen_expert_index[:, :, None] == ids).astype(jnp.bfloat16)
    named = jnp.sum(chosen, axis=1)
    below = jnp.asarray(np.tril(np.ones((row_count, row_count), np.float32), -1), jnp.bfloat16)
    rank = jnp.dot(below, named, preferred_element_type=jnp.float32).astype(jnp.int32)
    per_expert_group = experts // EXPERT_GROUPS
    group_of = jnp.asarray(np.repeat(np.eye(EXPERT_GROUPS, dtype=np.float32), per_expert_group, axis=1))
    group_weight = jnp.sum(expert_group_weight[:, :, None] * group_of[None], axis=1)
    weight = group_weight * jnp.sum(
        chosen.astype(jnp.float32) * chosen_expert_weight[:, :, None], axis=1
    )
    hot = (rank[:, :, None] == jnp.arange(capacity, dtype=jnp.int32)) & (named[:, :, None] > 0)
    pick = hot.astype(jnp.bfloat16).reshape(row_count, experts * capacity)
    route = jnp.where(hot, weight[:, :, None], 0.0).reshape(row_count, experts * capacity)
    route_high = route.astype(jnp.bfloat16)
    route_low = (route - route_high.astype(jnp.float32)).astype(jnp.bfloat16)
    outgoing = lax.dot_general(
        pick, ffn_in, (((0,), (0,)), ((), ())), preferred_element_type=jnp.float32
    ).astype(jnp.bfloat16)
    received = lax.all_to_all(
        outgoing.reshape(experts, capacity, width), ("sp", "tp"), split_axis=0, concat_axis=0,
        tiled=True,
    )
    flat_rows = received.reshape(-1, width)
    gate_part = jnp.dot(flat_rows, expert_gate_weight[0], preferred_element_type=jnp.float32)
    upward = jnp.dot(flat_rows, expert_up_weight[0], preferred_element_type=jnp.float32)
    hidden = (jax.nn.silu(gate_part) * upward).astype(jnp.bfloat16)
    finished = jnp.dot(
        hidden, expert_down_weight[0], preferred_element_type=jnp.float32
    ).astype(jnp.bfloat16)
    returned = lax.all_to_all(
        finished.reshape(received.shape), ("sp", "tp"), split_axis=0, concat_axis=0, tiled=True
    ).reshape(experts * capacity, width)
    summed = (
        mixed_rows.astype(jnp.float32)
        + jnp.dot(route_high, returned, preferred_element_type=jnp.float32)
        + jnp.dot(route_low, returned, preferred_element_type=jnp.float32)
    )
    return summed.astype(jnp.bfloat16)


def solution(mesh):
    placed = (
        P("sp", "tp"),
        P("sp", "tp"),
        P("sp", "tp"),
        P("sp", "tp"),
        P("sp", "tp"),
        P("sp", "tp"),
        P("tp"),
        P("tp"),
        P(None, "tp"),
        P(None, "tp"),
        P(None, "tp"),
        P("sp"),
        P(),
        P(("sp", "tp"), None),
        P(),
        P(),
        P(("sp", "tp"), None),
        P(("sp", "tp"), None),
        P(("sp", "tp"), None),
        P(("sp", "tp"), None, None),
        P(("sp", "tp"), None, None),
        P(("sp", "tp"), None, None),
    )
    return jax.shard_map(
        local, mesh=mesh, in_specs=placed, out_specs=P(("sp", "tp"), None), check_vma=False
    )
```

```python
import functools

import jax
import jax.numpy as jnp
import numpy as np
from jax import lax
from jax.experimental import pallas as pl
from jax.experimental.pallas import tpu as pltpu
from jax.sharding import PartitionSpec as P

D_STATE = 128
EXPERT_GROUPS = 4
LONGEST = 1536
EPSILON = 1e-06

NEG = -1e30
MESH_ID = pl.DeviceIdType.MESH
HOSTS = 4


def softplus(v):
    return jnp.maximum(v, 0.0) + jnp.log1p(jnp.exp(-jnp.abs(v)))


def silu(v):
    return v / (1.0 + jnp.exp(-v))


def exact_dot(a, b):
    return jnp.dot(a, b, preferred_element_type=jnp.float32, precision=lax.Precision.HIGHEST)


def mixer_kernel(
    n, greet, begin, x_hbm, b_hbm, c_hbm, gate_hbm, resid_hbm, w_hbm,
    step_ref, extra_ref, docrow_ref, rate_ref, direct_ref, taps_ref, btaps_ref, ctaps_ref,
    gain_ref, gain2_ref,
    mixed_ref, ffn_ref,
    x_ref, b_ref, c_ref, gate_ref, resid_ref, w_ref, docs_ref, pad, pad_docs,
    edge_x, edge_b, edge_c, edge_d,
    vconv, bconv, cconv, ylocal, cumx, t0, g0, rs, rg, tot, grow, rt, rgrow, hs, incoming,
    gated, regrouped,
    wsem, send, recv,
):
    sp = lax.axis_index("sp")
    tp = lax.axis_index("tp")
    length, channels = x_ref.shape
    state = b_ref.shape[1]
    lanes = 128
    chunks = channels // lanes
    heads = step_ref.shape[0]
    half = length // 2
    edge = edge_x.shape[0]
    hosts, _, block = rs.shape
    member = sp % hosts
    base_sp = sp - member

    loads = [
        pltpu.make_async_copy(source, target, wsem.at[i])
        for i, (source, target) in enumerate((
            (x_hbm, x_ref), (b_hbm, b_ref), (c_hbm, c_ref), (gate_hbm, gate_ref),
            (resid_hbm, resid_ref), (w_hbm, w_ref),
        ))
    ]
    for load in loads:
        load.start()

    docs_row = docrow_ref[...].astype(jnp.float32) + 1.0
    docs_ref[...] = jnp.transpose(jnp.broadcast_to(docs_row, (lanes, length)))

    barrier = pltpu.get_barrier_semaphore()
    count = jnp.int32(hosts)
    pl.semaphore_signal(barrier, inc=1, device_id=(sp, 1 - tp), device_id_type=MESH_ID)
    for d in range(1, hosts):
        pl.semaphore_signal(
            barrier, inc=1, device_id=(base_sp + (member + d) % hosts, tp), device_id_type=MESH_ID
        )
    for off in (1, hosts, 2 * hosts):
        @pl.when(sp + off < n)
        def _():
            pl.semaphore_signal(barrier, inc=1, device_id=(sp + off, tp), device_id_type=MESH_ID)

        @pl.when(sp >= off)
        def _():
            pl.semaphore_signal(barrier, inc=1, device_id=(sp - off, tp), device_id_type=MESH_ID)

        count = count + (sp + off < n).astype(jnp.int32) + (sp >= off).astype(jnp.int32)
    if greet is not None:
        count = count + greet(barrier)
    pl.semaphore_wait(barrier, count)

    def remote(sent, received, src, dst, device):
        return pltpu.make_async_remote_copy(
            src_ref=src, dst_ref=dst, send_sem=send.at[sent], recv_sem=recv.at[received],
            device_id=(device, tp), device_id_type=MESH_ID,
        )

    def copy(slot, src, dst, off):
        return remote(slot, slot, src, dst, sp + off)

    def part_of(i):
        return pl.ds(pl.multiple_of(i * block, block), block)

    def give(i, source):
        return [
            remote(4 + i, 4 + source, t0.at[:, part_of(i)], rs.at[source], base_sp + i),
            remote(
                4 + hosts + i, 4 + hosts + source, g0.at[:, part_of(i)], rg.at[source], base_sp + i
            ),
        ]

    def enter(i, source):
        return remote(
            4 + 2 * hosts + i, 4 + 2 * hosts + source, hs.at[i], incoming.at[:, part_of(source)],
            base_sp + i,
        )

    others = [(member + d) % hosts for d in range(1, hosts)]

    last = pl.ds(length - edge, edge)
    edges = [
        copy(0, x_ref.at[last, :], edge_x, 1),
        copy(1, b_ref.at[last, :], edge_b, 1),
        copy(2, c_ref.at[last, :], edge_c, 1),
        copy(3, docs_ref.at[last, :], edge_d, 1),
    ]

    def start(copies, off):
        @pl.when(sp + off < n)
        def _():
            for one in copies:
                one.start()

    def wait_recv(copies, off):
        @pl.when(sp >= off)
        def _():
            for one in copies:
                one.wait_recv()

    def wait_send(copies, off):
        @pl.when(sp + off < n)
        def _():
            for one in copies:
                one.wait_send()

    for load in loads[:3]:
        load.wait()
    start(edges, 1)
    if begin is not None:
        begin()

    head_row = lax.broadcasted_iota(jnp.int32, (heads, heads), 0)
    head_col = lax.broadcasted_iota(jnp.int32, (heads, heads), 1)

    def column(ref):
        return jnp.sum(jnp.where(head_row == head_col, ref[...], 0.0), axis=1, keepdims=True)

    direct_column = column(direct_ref)
    step = softplus(step_ref[...])
    logs = extra_ref[...] - step * column(rate_ref)
    rows = lax.broadcasted_iota(jnp.int32, (length, length), 0)
    cols = lax.broadcasted_iota(jnp.int32, (length, length), 1)
    causal = rows >= cols
    cum = lax.dot_general(
        causal.astype(jnp.float32), logs, (((1,), (1,)), ((), ())),
        preferred_element_type=jnp.float32, precision=lax.Precision.HIGHEST,
    )
    cum_t = exact_dot(logs, (rows <= cols).astype(jnp.float32))
    same = docs_ref[:, 0:1] == docs_row
    blocked = jnp.where(causal & same, 0.0, NEG)
    tail = (docs_ref[...] == docs_ref[length - 1 : length, :]).astype(jnp.float32)

    pad[edge:, :channels] = x_ref[...].astype(jnp.float32)
    pad[edge:, channels : channels + state] = b_ref[...].astype(jnp.float32)
    pad[edge:, channels + state :] = c_ref[...].astype(jnp.float32)
    pad_docs[edge:, :] = docs_ref[...]

    wait_recv(edges, 1)
    has = sp >= 1
    pad[:edge, :channels] = jnp.where(has, edge_x[...].astype(jnp.float32), 0.0)
    pad[:edge, channels : channels + state] = jnp.where(has, edge_b[...].astype(jnp.float32), 0.0)
    pad[:edge, channels + state :] = jnp.where(has, edge_c[...].astype(jnp.float32), 0.0)
    pad_docs[:edge, :] = jnp.where(has, edge_d[...], 0.0)

    taps_count = taps_ref.shape[0]
    base = edge - taps_count + 1
    masks = [
        (pad_docs[base + k : base + k + length, :] == docs_ref[...]).astype(jnp.float32)
        for k in range(taps_count - 1)
    ]

    def conv(at, taps, start_lane):
        total = taps[taps_count - 1 :, start_lane : start_lane + lanes].astype(
            jnp.float32
        ) * pad[edge : edge + length, at : at + lanes]
        for k in range(taps_count - 1):
            total = total + (
                taps[k : k + 1, start_lane : start_lane + lanes].astype(jnp.float32)
                * pad[base + k : base + k + length, at : at + lanes]
                * masks[k]
            )
        return silu(total).astype(jnp.bfloat16)

    bconv[...] = conv(channels, btaps_ref, 0)
    cconv[...] = conv(channels + state, ctaps_ref, 0)

    keep = (docs_ref[length - 1 : length, :] == pad_docs[edge - 1 : edge, :]).astype(jnp.float32)
    keep = keep * has.astype(jnp.float32)
    b_t = jnp.transpose(bconv[...].astype(jnp.float32)).astype(jnp.bfloat16)
    per_chunk = heads // chunks
    width = lanes // per_chunk
    spread_row = lax.broadcasted_iota(jnp.int32, (heads, lanes), 0) * width
    spread_lane = lax.broadcasted_iota(jnp.int32, (heads, lanes), 1)

    def widen(j):
        at = spread_lane + j * lanes - spread_row
        return jnp.where((at >= 0) & (at < width), 1.0, 0.0)

    lane = lax.broadcasted_iota(jnp.int32, (length, lanes), 1)
    step_columns = jnp.transpose(
        jnp.concatenate([step, jnp.zeros((lanes - heads, length), jnp.float32)], axis=0)
    )

    def spread(columns, j):
        result = None
        for k in range(per_chunk):
            h = j * per_chunk + k
            part = jnp.broadcast_to(columns[:, h : h + 1], (length, lanes))
            result = part if result is None else jnp.where(lane < k * width, result, part)
        return result

    for j in range(chunks):
        at = slice(j * lanes, (j + 1) * lanes)
        value = conv(j * lanes, taps_ref, j * lanes)
        vconv[:, at] = value
        cum_wide = spread(cum, j)
        cumx[:, at] = cum_wide
        step_wide = spread(step_columns, j)
        stepped = (step_wide * value.astype(jnp.float32)).astype(jnp.bfloat16)
        ylocal[:, at] = stepped.astype(jnp.float32)
        ending = cum_wide[length - 1 : length, :]
        ended = (jnp.exp(ending - cum_wide) * tail * stepped.astype(jnp.float32)).astype(
            jnp.bfloat16
        )
        t0[:, at] = jnp.dot(b_t, ended, preferred_element_type=jnp.float32).astype(jnp.bfloat16)
        g0[:, at] = jnp.broadcast_to(jnp.exp(ending) * keep, (8, lanes))
        i = j * lanes // block
        if (j + 1) * lanes == (i + 1) * block:
            @pl.when(member != i)
            def _():
                for one in give(i, member):
                    one.start()

            @pl.when(member == i)
            def _():
                rs[i] = t0[:, i * block : (i + 1) * block]
                rg[i] = g0[:, i * block : (i + 1) * block]

    scores = lax.dot_general(
        cconv[...], bconv[...], (((1,), (1,)), ((), ())), preferred_element_type=jnp.float32
    )

    def inside(j):
        at = slice(j * lanes, (j + 1) * lanes)
        stepped = ylocal[:, at].astype(jnp.bfloat16)
        result = None
        for k in range(per_chunk):
            h = j * per_chunk + k
            decay = jnp.exp(cum[:, h : h + 1] - cum_t[h : h + 1, :] + blocked)
            part = jnp.dot(
                (scores * decay).astype(jnp.bfloat16), stepped, preferred_element_type=jnp.float32
            )
            result = part if result is None else jnp.where(lane < k * width, result, part)
        direct = jnp.sum(widen(j) * direct_column, axis=0, keepdims=True)
        ylocal[:, at] = result + direct * vconv[:, at].astype(jnp.float32)

    early = chunks // 4
    late = chunks * 5 // 8
    for j in range(early):
        inside(j)

    for i in others:
        for one in give(i, i):
            one.wait_recv()
    total = jnp.zeros((state, block), jnp.float32)
    growth = jnp.ones((1, block), jnp.float32)
    for i in range(hosts):
        factor = rg[i][0:1, :]
        total = rs[i].astype(jnp.float32) + factor * total
        growth = growth * factor
    tot[...] = total.astype(jnp.bfloat16)
    grow[...] = jnp.broadcast_to(growth, grow.shape)
    slot = 4 + 3 * hosts
    nearer = [copy(slot, tot, rt.at[0], hosts), copy(slot + 1, grow, rgrow, hosts)]
    further = [copy(slot + 2, tot, rt.at[1], 2 * hosts)]
    start(nearer, hosts)
    start(further, 2 * hosts)
    for j in range(early, late):
        inside(j)

    wait_recv(nearer, hosts)
    wait_recv(further, 2 * hosts)
    carried = jnp.where(sp >= 2 * hosts, rt[1].astype(jnp.float32), 0.0)
    carried = jnp.where(sp >= hosts, rt[0].astype(jnp.float32) + rgrow[0:1, :] * carried, 0.0)
    for i in range(hosts):
        @pl.when(member != i)
        def _():
            hs[i] = carried.astype(jnp.bfloat16)
            enter(i, member).start()

        @pl.when(member == i)
        def _():
            incoming[:, i * block : (i + 1) * block] = carried.astype(jnp.bfloat16)

        if i < hosts - 1:
            carried = rs[i].astype(jnp.float32) + rg[i][0:1, :] * carried
    for j in range(late, chunks):
        inside(j)

    for i in others:
        enter(i, i).wait_recv()
    loads[3].wait()
    entering = (docs_ref[...] == pad_docs[edge - 1 : edge, :]).astype(jnp.float32)
    for j in range(chunks):
        at = slice(j * lanes, (j + 1) * lanes)
        readout = jnp.dot(cconv[...], incoming[:, at], preferred_element_type=jnp.float32)
        whole = ylocal[:, at] + readout * jnp.exp(cumx[:, at]) * entering
        gated[:, at] = (whole * silu(gate_ref[:, at].astype(jnp.float32))).astype(jnp.bfloat16)

    swap = pltpu.make_async_remote_copy(
        src_ref=gated.at[pl.ds(pl.multiple_of((1 - tp) * half, half), half), :],
        dst_ref=regrouped,
        send_sem=send.at[slot + 3], recv_sem=recv.at[slot + 3],
        device_id=(sp, 1 - tp), device_id_type=MESH_ID,
    )
    swap.start()
    wait_send(edges, 1)
    wait_send(nearer, hosts)
    wait_send(further, 2 * hosts)
    for i in others:
        for one in give(i, member):
            one.wait_send()
        enter(i, member).wait_send()
    loads[4].wait()
    loads[5].wait()
    swap.wait()
    own = gated[pl.ds(pl.multiple_of(tp * half, half), half), :].astype(jnp.float32)
    other = regrouped[...].astype(jnp.float32)
    total = jnp.sum(own * own, axis=-1, keepdims=True) + jnp.sum(other * other, axis=-1, keepdims=True)
    features = 2 * channels
    factor = lax.rsqrt(total / features + EPSILON)
    low = jnp.where(tp == 0, own, other)
    high = jnp.where(tp == 0, other, own)
    low = (low * factor * gain_ref[:, :channels]).astype(jnp.bfloat16)
    high = (high * factor * gain_ref[:, channels:]).astype(jnp.bfloat16)
    square = jnp.zeros((half, 1), jnp.float32)
    piece = 512
    model = resid_ref.shape[1]
    for j in range(model // piece):
        at = slice(j * piece, (j + 1) * piece)
        projected = jnp.dot(low, w_ref[:channels, at], preferred_element_type=jnp.float32)
        projected += jnp.dot(high, w_ref[channels:, at], preferred_element_type=jnp.float32)
        mixed = (resid_ref[:, at].astype(jnp.float32) + projected).astype(jnp.bfloat16)
        mixed_ref[:, at] = mixed
        wide = mixed.astype(jnp.float32)
        square += jnp.sum(wide * wide, axis=-1, keepdims=True)
    factor = lax.rsqrt(square / model + EPSILON)
    ffn_ref[...] = (mixed_ref[...].astype(jnp.float32) * factor * gain2_ref[...]).astype(jnp.bfloat16)


def mixer_operands(x, b, c, gate, step, extra, rate, direct, taps, btaps, ctaps, docs, gain, resid,
                   weight, gain2):
    return (x, b, c, gate, resid, weight), (
        step.T, extra.T, docs[None, :], rate[None, :], direct[None, :], taps, btaps, ctaps,
        gain[None, :], gain2[None, :],
    )


def mixer_scratch(n, x, b, c, gate, resid, weight):
    length, channels = x.shape
    state = b.shape[1]
    half = resid.shape[0]
    hosts = HOSTS
    block = channels // hosts
    assert state == D_STATE and n % hosts == 0 and block % 128 == 0
    assert (LONGEST - 2) // (hosts * length) + 1 <= 2
    bf, f32 = jnp.bfloat16, jnp.float32
    edge = 16
    vm = pltpu.VMEM
    sems = 4 + 3 * hosts + 4
    return [
        vm(x.shape, bf), vm(b.shape, bf), vm(c.shape, bf), vm(gate.shape, bf),
        vm(resid.shape, bf), vm(weight.shape, bf), vm((length, 128), f32),
        vm((edge + length, channels + 2 * state), f32), vm((edge + length, 128), f32),
        vm((edge, channels), bf), vm((edge, state), bf), vm((edge, state), bf),
        vm((edge, 128), f32),
        vm((length, channels), bf), vm((length, state), bf), vm((length, state), bf),
        vm((length, channels), f32), vm((length, channels), f32),
        vm((state, channels), bf), vm((8, channels), f32),
        vm((hosts, state, block), bf), vm((hosts, 8, block), f32),
        vm((state, block), bf), vm((8, block), f32),
        vm((2, state, block), bf), vm((8, block), f32),
        vm((hosts, state, block), bf), vm((state, channels), bf),
        vm((length, channels), bf), vm((half, channels), bf),
        pltpu.SemaphoreType.DMA((6,)), pltpu.SemaphoreType.DMA((sems,)),
        pltpu.SemaphoreType.DMA((sems,)),
    ]


def mixer(n, operands):
    large, small = mixer_operands(*operands)
    return pl.pallas_call(
        functools.partial(mixer_kernel, n, None, None),
        out_shape=[jax.ShapeDtypeStruct(large[4].shape, jnp.bfloat16)] * 2,
        in_specs=[pl.BlockSpec(memory_space=pl.ANY)] * len(large)
        + [pl.BlockSpec(memory_space=pltpu.VMEM)] * len(small),
        out_specs=[pl.BlockSpec(memory_space=pltpu.VMEM)] * 2,
        scratch_shapes=mixer_scratch(n, *large),
        compiler_params=pltpu.CompilerParams(
            collective_id=0, has_side_effects=True, vmem_limit_bytes=58 * 1024 * 1024
        ),
    )(*large, *small)


def layer_kernel(planes, tps, large, small, *refs):
    mixer_in = refs[: large + small]
    refs = refs[large + small :]
    ids_ref, group_ref, weight_ref, wg_hbm, wu_hbm, wd_hbm, out_ref = refs[:7]
    (
        mixed_ref, wg, wu, wd, meta, picks, routes, line, slots, arrived, done, back, part, mine,
        parts,
        wsem, msend, mrecv, lsend, lrecv, fsend, frecv, bsend, brecv, psend, precv,
    ) = refs[7:33]
    mixer_scratch_refs = refs[33:]
    sp = lax.axis_index("sp")
    tp = lax.axis_index("tp")
    rows, model = mixed_ref.shape
    per = lax.axis_size("sp") * tps // planes
    hosts = per // tps
    cap = rows // per
    experts = planes * per
    chunks = lrecv.shape[1]
    width = model // chunks
    z = sp // hosts
    q = (sp % hosts) * tps + tp

    loads = [
        pltpu.make_async_copy(wg_hbm.at[0], wg, wsem.at[0]),
        pltpu.make_async_copy(wu_hbm.at[0], wu, wsem.at[1]),
        pltpu.make_async_copy(wd_hbm.at[0], wd, wsem.at[2]),
    ]

    def place(plane, member):
        return (plane * hosts + member // tps, member % tps)

    def loop(low, high, act):
        def body(k, carry):
            act(k)
            return carry

        lax.fori_loop(low, high, body, 0)

    def greet(barrier):
        def signal(device):
            pl.semaphore_signal(barrier, inc=1, device_id=device, device_id_type=MESH_ID)

        loop(1, per, lambda d: signal(place(z, (q + d) % per)))
        loop(1, planes, lambda d: signal(place((z + d) % planes, q)))
        return per + planes - 2

    def columns(c):
        return pl.ds(pl.multiple_of(c * width, width), width)

    def member_rows(member):
        return pl.ds(pl.multiple_of(member * cap, cap), cap)

    def tell(plane, target):
        return pltpu.make_async_remote_copy(
            src_ref=meta.at[plane], dst_ref=meta.at[plane],
            send_sem=msend.at[target], recv_sem=mrecv.at[plane],
            device_id=place(target, q), device_id_type=MESH_ID,
        )

    def hop(plane, c, up):
        return pltpu.make_async_remote_copy(
            src_ref=line.at[plane, :, columns(c)], dst_ref=line.at[plane, :, columns(c)],
            send_sem=lsend.at[up, plane, c], recv_sem=lrecv.at[plane, c],
            device_id=place(z + 2 * up - 1, q), device_id_type=MESH_ID,
        )

    peers = [
        ((q + d) % per, place(z, (q + d) % per)) for d in range(1, per)
    ]

    def forward(plane, c, peer):
        member, device = peer
        return pltpu.make_async_remote_copy(
            src_ref=slots.at[plane, member_rows(member), columns(c)],
            dst_ref=arrived.at[plane, member_rows(q), columns(c)],
            send_sem=fsend.at[plane], recv_sem=frecv.at[plane],
            device_id=device, device_id_type=MESH_ID,
        )

    def backward(plane, c, peer):
        member, device = peer
        return pltpu.make_async_remote_copy(
            src_ref=done.at[plane, member_rows(member), columns(c)],
            dst_ref=back.at[plane, member_rows(q), columns(c)],
            send_sem=bsend.at[plane], recv_sem=brecv.at[plane, c],
            device_id=device, device_id_type=MESH_ID,
        )

    def home(plane, c, up):
        landing = jnp.where((up == 0) & (plane == z - 1), planes, plane)
        return pltpu.make_async_remote_copy(
            src_ref=part.at[plane, :, columns(c)], dst_ref=parts.at[landing, :, columns(c)],
            send_sem=psend.at[plane, c], recv_sem=precv.at[landing, c],
            device_id=place(z + 2 * up - 1, q), device_id_type=MESH_ID,
        )

    def homed(landing, c):
        view = parts.at[landing, :, columns(c)]
        return pltpu.make_async_copy(view, view, precv.at[landing, c])

    others = pl.ds(0, (per - 1) * cap)

    def whole(ref, plane, sem):
        view = ref.at[plane, others, :]
        return pltpu.make_async_copy(view, view, sem.at[plane])

    def slab(plane, c):
        view = back.at[plane, others, columns(c)]
        return pltpu.make_async_copy(view, view, brecv.at[plane, c])

    choose = ids_ref.shape[0]

    def begin():
        for load in loads:
            load.start()
        ids = ids_ref[...]
        group_size = experts // EXPERT_GROUPS
        weight = jnp.zeros(ids.shape, jnp.float32)
        for g in range(EXPERT_GROUPS):
            inside = (ids >= g * group_size) & (ids < (g + 1) * group_size)
            weight = weight + jnp.where(inside, group_ref[g : g + 1, :], 0.0)
        meta[z] = jnp.concatenate(
            [
                ids.astype(jnp.float32), weight * weight_ref[...],
                jnp.zeros((meta.shape[1] - 2 * choose, rows), jnp.float32),
            ],
            axis=0,
        )
        loop(1, planes, lambda d: tell(z, (z + d) % planes).start())

    mixer_kernel(
        lax.axis_size("sp"), greet, begin, *mixer_in, mixed_ref, line.at[z], *mixer_scratch_refs
    )
    for c in range(chunks):
        @pl.when(z < planes - 1)
        def _():
            hop(z, c, 1).start()

        @pl.when(z > 0)
        def _():
            hop(z, c, 0).start()

    slot_member = lax.broadcasted_iota(jnp.int32, (per, cap, rows), 0).reshape(rows, rows)
    slot_place = lax.broadcasted_iota(jnp.int32, (per, cap, rows), 1).reshape(rows, rows)
    slot_expert = (slot_member + z * per).astype(jnp.float32)
    slot_place = slot_place.astype(jnp.float32)
    earlier = (
        lax.broadcasted_iota(jnp.int32, (rows, rows), 0)
        < lax.broadcasted_iota(jnp.int32, (rows, rows), 1)
    ).astype(jnp.bfloat16)

    def sort_out(plane):
        known = meta[plane]
        named = jnp.zeros((rows, rows), jnp.float32)
        value = jnp.zeros((rows, rows), jnp.float32)
        for k in range(choose):
            chosen = (known[k : k + 1, :] == slot_expert).astype(jnp.float32)
            named = named + chosen
            value = value + chosen * known[choose + k : choose + k + 1, :]
        rank = jnp.dot(named.astype(jnp.bfloat16), earlier, preferred_element_type=jnp.float32)
        hot = jnp.where(rank == slot_place, named, 0.0)
        picks[plane] = hot.astype(jnp.bfloat16)
        routes[plane] = jnp.transpose(hot * value).astype(jnp.bfloat16)

    lag = chunks + 1

    def stage_rows(k, c, up, plane):
        @pl.when(k > 0)
        def _():
            hop(plane, c, up).wait_recv()

            @pl.when((up == 0) & (z < planes - 1))
            def _():
                hop(plane, c, 1).start()

            @pl.when((up == 1) & (z > 0))
            def _():
                hop(plane, c, 0).start()

        @pl.when(c == 0)
        def _():
            @pl.when(k > 0)
            def _():
                tell(plane, plane).wait_recv()

            sort_out(plane)

        at = columns(c)
        slots[plane, :, at] = jnp.dot(
            picks[plane], line[plane, :, at], preferred_element_type=jnp.float32
        ).astype(jnp.bfloat16)
        arrived[plane, member_rows(q), at] = slots[plane, member_rows(q), at]
        for peer in peers:
            forward(plane, c, peer).start()

    def stage_experts(k, plane):
        @pl.when(k == 0)
        def _():
            for load in loads:
                load.wait()

        whole(arrived, plane, frecv).wait()
        tokens = arrived[plane]
        gate = jnp.dot(tokens, wg[...], preferred_element_type=jnp.float32)
        up = jnp.dot(tokens, wu[...], preferred_element_type=jnp.float32)
        hidden = (silu(gate) * up).astype(jnp.bfloat16)
        for c in range(chunks):
            at = slice(c * width, (c + 1) * width)
            done[plane, :, at] = jnp.dot(
                hidden, wd[:, at], preferred_element_type=jnp.float32
            ).astype(jnp.bfloat16)
            back[plane, member_rows(q), at] = done[plane, member_rows(q), at]
            for peer in peers:
                backward(plane, c, peer).start()

    def stage_home(k, c, plane):
        slab(plane, c).wait()
        at = columns(c)
        total = jnp.dot(
            routes[plane], back[plane, :, at], preferred_element_type=jnp.float32
        )

        @pl.when(k == 0)
        def _():
            mine[:, at] = total

        @pl.when(k > 0)
        def _():
            part[plane, :, at] = total.astype(jnp.bfloat16)

        @pl.when((z == 0) & (k > 0))
        def _():
            home(plane, c, 1).start()

        @pl.when((z == planes - 1) & (k > 0))
        def _():
            home(plane, c, 0).start()

    def tick(v):
        def both(k, act):
            def side(up):
                plane = z + k * (2 * up - 1)

                @pl.when((plane >= 0) & (plane < planes) & ((k > 0) | (up == 0)))
                def _():
                    act(up, plane)

            loop(0, 2, side)

        @pl.when(v < planes * chunks)
        def _():
            k = v // chunks
            c = v % chunks
            both(k, lambda up, plane: stage_rows(k, c, up, plane))

        @pl.when((v % chunks == 0) & (v >= chunks) & (v <= planes * chunks))
        def _():
            k = v // chunks - 1
            both(k, lambda up, plane: stage_experts(k, plane))

        @pl.when(v >= lag)
        def _():
            k = (v - lag) // chunks
            c = (v - lag) % chunks
            both(k, lambda up, plane: stage_home(k, c, plane))

    loop(0, planes * chunks + lag, tick)

    def pass_on(plane, c, up):
        at = columns(c)
        homed(plane, c).wait()
        part[plane, :, at] = (
            part[plane, :, at].astype(jnp.float32) + parts[plane, :, at].astype(jnp.float32)
        ).astype(jnp.bfloat16)
        home(plane, c, up).start()

    behind = 1

    def relay(v):
        def serve(w, up):
            reach = 1 + w // chunks
            plane = jnp.where(up == 1, reach, planes - 1 - reach)
            valid = jnp.where(up == 1, (plane > z) & (z > 0), (plane < z) & (z < planes - 1))

            @pl.when(valid & (w >= 0) & (w < (planes - 1) * chunks))
            def _():
                pass_on(plane, w % chunks, up)

        leading = jnp.where(2 * z < planes, 1, 0)
        loop(0, 2, lambda i: serve(v - i * behind, jnp.where(i == 0, leading, 1 - leading)))

    loop(0, (planes - 1) * chunks + behind, relay)

    for c in range(chunks):
        at = slice(c * width, (c + 1) * width)
        mine[:, at] = mine[:, at] + mixed_ref[:, at].astype(jnp.float32)

        def add(landing):
            homed(landing, c).wait()
            mine[:, at] = mine[:, at] + parts[landing, :, at].astype(jnp.float32)

        @pl.when(z > 0)
        def _():
            add(z)

        @pl.when(z < planes - 1)
        def _():
            add(planes)

        out_ref[:, at] = mine[:, at].astype(jnp.bfloat16)

    loop(1, planes, lambda d: tell(z, (z + d) % planes).wait_send())

    def finish(plane):
        whole(slots, plane, fsend).wait()
        whole(done, plane, bsend).wait()

        def each(c):
            @pl.when((plane <= z) & (z < planes - 1))
            def _():
                hop(plane, c, 1).wait_send()

            @pl.when((plane >= z) & (z > 0))
            def _():
                hop(plane, c, 0).wait_send()

            @pl.when(plane != z)
            def _():
                home(plane, c, 1).wait_send()

        loop(0, chunks, each)

    loop(0, planes, finish)


def layer(n, operands, ids, group_weight, chosen_weight, gate_weight, up_weight, down_weight,
          planes):
    large, small = mixer_operands(*operands)
    rows, model = large[4].shape
    chunks = 4
    bf, f32 = jnp.bfloat16, jnp.float32
    vm = pltpu.VMEM
    dma = pltpu.SemaphoreType.DMA
    return pl.pallas_call(
        functools.partial(layer_kernel, planes, lax.axis_size("tp"), len(large), len(small)),
        out_shape=jax.ShapeDtypeStruct((rows, model), bf),
        in_specs=[pl.BlockSpec(memory_space=pl.ANY)] * len(large)
        + [pl.BlockSpec(memory_space=pltpu.VMEM)] * (len(small) + 3)
        + [pl.BlockSpec(memory_space=pl.ANY)] * 3,
        out_specs=pl.BlockSpec(memory_space=pltpu.VMEM),
        scratch_shapes=[
            vm((rows, model), bf),
            vm(gate_weight.shape[1:], bf), vm(up_weight.shape[1:], bf),
            vm(down_weight.shape[1:], bf),
            vm((planes, 8, rows), f32),
            vm((planes, rows, rows), bf), vm((planes, rows, rows), bf),
            vm((planes, rows, model), bf), vm((planes, rows, model), bf),
            vm((planes, rows, model), bf), vm((planes, rows, model), bf),
            vm((planes, rows, model), bf), vm((planes, rows, model), bf),
            vm((rows, model), f32), vm((planes + 1, rows, model), bf),
            dma((3,)), dma((planes,)), dma((planes,)),
            dma((2, planes, chunks)), dma((planes, chunks)),
            dma((planes,)), dma((planes,)), dma((planes,)), dma((planes, chunks)),
            dma((planes, chunks)), dma((planes + 1, chunks)),
        ] + mixer_scratch(n, *large),
        compiler_params=pltpu.CompilerParams(
            collective_id=1, has_side_effects=True, vmem_limit_bytes=62 * 1024 * 1024
        ),
    )(*large, *small, ids, group_weight, chosen_weight, gate_weight, up_weight, down_weight)


def local(
    mixer_value_rows,
    input_map_rows,
    output_map_rows,
    gate_preactivation,
    step_preactivation,
    position_extra_decay,
    head_decay_rate,
    head_direct_term,
    value_taps,
    input_map_taps,
    output_map_taps,
    document_index,
    gated_norm_gain,
    residual,
    mixer_output_weight,
    expert_norm_gain,
    expert_group_weight,
    chosen_expert_weight,
    chosen_expert_index,
    expert_gate_weight,
    expert_up_weight,
    expert_down_weight,
):
    operands = (
        mixer_value_rows, input_map_rows, output_map_rows, gate_preactivation, step_preactivation,
        position_extra_decay, head_decay_rate, head_direct_term, value_taps, input_map_taps,
        output_map_taps, document_index, gated_norm_gain, residual, mixer_output_weight,
        expert_norm_gain,
    )
    hosts, tps = lax.axis_size("sp"), lax.axis_size("tp")
    experts = hosts * tps
    row_count, width = residual.shape
    choose = chosen_expert_index.shape[1]
    capacity = 2 * mixer_value_rows.shape[0] // experts
    per = row_count // capacity
    if (
        capacity % 16 == 0 and row_count % capacity == 0 and experts % per == 0
        and per % tps == 0 and experts % EXPERT_GROUPS == 0 and choose <= 4 and experts >= 2 * per
    ):
        return layer(
            hosts, operands, chosen_expert_index.T, expert_group_weight.T, chosen_expert_weight.T,
            expert_gate_weight, expert_up_weight, expert_down_weight, experts // per,
        )
    mixed_rows, ffn_in = mixer(hosts, operands)
    ids = jnp.arange(experts, dtype=jnp.int32)
    chosen = (chosen_expert_index[:, :, None] == ids).astype(jnp.bfloat16)
    named = jnp.sum(chosen, axis=1)
    below = jnp.asarray(np.tril(np.ones((row_count, row_count), np.float32), -1), jnp.bfloat16)
    rank = jnp.dot(below, named, preferred_element_type=jnp.float32).astype(jnp.int32)
    per_expert_group = experts // EXPERT_GROUPS
    group_of = jnp.asarray(np.repeat(np.eye(EXPERT_GROUPS, dtype=np.float32), per_expert_group, axis=1))
    group_weight = jnp.sum(expert_group_weight[:, :, None] * group_of[None], axis=1)
    weight = group_weight * jnp.sum(
        chosen.astype(jnp.float32) * chosen_expert_weight[:, :, None], axis=1
    )
    hot = (rank[:, :, None] == jnp.arange(capacity, dtype=jnp.int32)) & (named[:, :, None] > 0)
    pick = hot.astype(jnp.bfloat16).reshape(row_count, experts * capacity)
    route = jnp.where(hot, weight[:, :, None], 0.0).reshape(row_count, experts * capacity)
    route_high = route.astype(jnp.bfloat16)
    route_low = (route - route_high.astype(jnp.float32)).astype(jnp.bfloat16)
    outgoing = lax.dot_general(
        pick, ffn_in, (((0,), (0,)), ((), ())), preferred_element_type=jnp.float32
    ).astype(jnp.bfloat16)
    received = lax.all_to_all(
        outgoing.reshape(experts, capacity, width), ("sp", "tp"), split_axis=0, concat_axis=0,
        tiled=True,
    )
    flat_rows = received.reshape(-1, width)
    gate_part = jnp.dot(flat_rows, expert_gate_weight[0], preferred_element_type=jnp.float32)
    upward = jnp.dot(flat_rows, expert_up_weight[0], preferred_element_type=jnp.float32)
    hidden = (jax.nn.silu(gate_part) * upward).astype(jnp.bfloat16)
    finished = jnp.dot(
        hidden, expert_down_weight[0], preferred_element_type=jnp.float32
    ).astype(jnp.bfloat16)
    returned = lax.all_to_all(
        finished.reshape(received.shape), ("sp", "tp"), split_axis=0, concat_axis=0, tiled=True
    ).reshape(experts * capacity, width)
    summed = (
        mixed_rows.astype(jnp.float32)
        + jnp.dot(route_high, returned, preferred_element_type=jnp.float32)
        + jnp.dot(route_low, returned, preferred_element_type=jnp.float32)
    )
    return summed.astype(jnp.bfloat16)


def solution(mesh):
    placed = (
        P("sp", "tp"),
        P("sp", "tp"),
        P("sp", "tp"),
        P("sp", "tp"),
        P("sp", "tp"),
        P("sp", "tp"),
        P("tp"),
        P("tp"),
        P(None, "tp"),
        P(None, "tp"),
        P(None, "tp"),
        P("sp"),
        P(),
        P(("sp", "tp"), None),
        P(),
        P(),
        P(("sp", "tp"), None),
        P(("sp", "tp"), None),
        P(("sp", "tp"), None),
        P(("sp", "tp"), None, None),
        P(("sp", "tp"), None, None),
        P(("sp", "tp"), None, None),
    )
    return jax.shard_map(
        local, mesh=mesh, in_specs=placed, out_specs=P(("sp", "tp"), None), check_vma=False
    )
```
